32 devices in a mesh: ep: 8 (over z, core), tp: 4 (over y, x).
Axes of the slice: x: 2, y: 2, z: 4, core: 2. Of those that a mesh axis runs over, the one named last changes fastest.
Arguments:
- tokens: bfloat16 [64, 2048], P('ep'), may hold values from -6 to 6
- attn_gain: float32 [2048], replicated, may hold values from 0.1 to 1.9
- query_weight: bfloat16 [2048, 4096], P('ep', 'tp'), may hold values from -0.125 to 0.125
- key_weight: bfloat16 [2048, 4096], P('ep', 'tp'), may hold values from -0.125 to 0.125
- value_weight: bfloat16 [2048, 4096], P('ep', 'tp'), may hold values from -0.125 to 0.125
- query_gain: float32 [128], replicated, may hold values from 0.1 to 1.9
- stick_bias: float32 [32], P('tp'), may hold values from -7 to -2.5
- key_cache: bfloat16 [64, 32, 512, 128], P('ep', 'tp'), may hold values from -6 to 6
- value_cache: bfloat16 [64, 32, 512, 128], P('ep', 'tp'), may hold values from -6 to 6
- lengths: int32 [64], P('ep'), may hold values from 64 to 512, as said below
- out_weight: bfloat16 [4096, 2048], P('tp'), may hold values from -0.375 to 0.375
- mix_gain: float32 [2048], replicated, may hold values from 0.1 to 1.9
- route_ids: int32 [64, 2], P('ep'), may hold values from 0 to 7, all different within a row; in each aligned block of 8 rows (0 to 7, 8 to 15, ...) at most 4 rows name the same one
- route_weights: float32 [64, 2], P('ep'), may hold values from 0.2 to 1
- expert_gate: bfloat16 [8, 2048, 2560], P('ep', None, 'tp'), may hold values from -0.125 to 0.125
- expert_up: bfloat16 [8, 2048, 2560], P('ep', None, 'tp'), may hold values from -0.125 to 0.125
- expert_down: bfloat16 [8, 2560, 2048], P('ep', 'tp'), may hold values from -0.15625 to 0.15625
- side_gate: bfloat16 [2048, 1024], P(None, 'tp'), may hold values from -0.125 to 0.125
- side_up: bfloat16 [2048, 1024], P(None, 'tp'), may hold values from -0.125 to 0.125
- side_down: bfloat16 [1024, 2048], P('tp'), may hold values from -0.25 to 0.25
- branch_gate: float32 [2048], replicated, may hold values from -0.125 to 0.125
Outputs:
- mixed: bfloat16 [64, 2048], P('ep', 'tp')
- new_keys: bfloat16 [64, 4096], P('ep', 'tp')
- new_values: bfloat16 [64, 4096], P('ep', 'tp')
The draws below stay inside these ranges and needn't reach their ends.
Inputs may be any that keep to these rules, and one draw needn't show every extreme that they name: `lengths`: at least an eighth of 512; the first sequence has 512. `route_ids`: each token names 2 different experts. In the rows of one device no expert is named by more than 4 rows, a bound that some block reaches of some device.
All inputs are finite; a program needn't handle non-finite values.
Results may differ from the reference program's by a relative error of at most 0.018.
Values may be sent and summed in bfloat16 or wider, within the bound.
A program may use at most 64 MiB of HBM per device.

```python
import math
import jax
import jax.numpy as jnp
import numpy as np
from jax import lax

D = 2048
H = 32
DH = 128
FF_E = 2560
SH = 1024
TOP = 2
SEQS = 8
L = 512
BATCH = 64
E = 8
CAP = 4
N_EP = 8


def draw_lengths(key, part):
    drawn = jax.random.randint(key, (BATCH,), L // 8, L + 1, dtype=jnp.int32)
    return drawn.at[0].set(L)


def raised(result, key, source, target, shards_of, factor):
    owner, partner = [(jnp.arange(result.shape[axis_at]) // (result.shape[axis_at] // shards_of)).reshape([-1 if axis == axis_at else 1 for axis in range(result.ndim)]) for axis_at in (source, target)]
    chosen = jax.random.permutation(key, shards_of)[partner]
    strong = (owner == chosen) | (owner == (partner + shards_of // 2) % shards_of)
    return jnp.where(strong, factor * result, result)


def level_of(key, dims, pieces, low, high):
    gain = 1.0
    for axis_at, parts in pieces:
        steps = jax.random.uniform(jax.random.fold_in(jax.random.fold_in(key, 6), axis_at), (parts,), jnp.float32, low / len(pieces), high / len(pieces))
        gain = gain * jnp.repeat(jnp.exp(steps), dims[axis_at] // parts).reshape((-1,) + (1,) * (len(dims) - 1 - axis_at))
    return gain


def routed_block(own_key, own, number, rows, amount, top, bound, lean):
    ranking = jax.random.permutation(own_key, amount)
    crowded, ordinary = portions_of(amount, rows * top, bound, lean, True), portions_of(amount, rows * top, bound, lean, False)
    places = jnp.arange(amount)

    def named(sizes, rotation):
        used = int((sizes > 0).sum())
        fixed = max(1, used // 4)
        moved = fixed + (places - fixed + rotation * (used - fixed)) % max(1, amount - fixed)
        return jnp.zeros((amount,), jnp.int32).at[ranking[jnp.where(places < fixed, places, moved)]].set(jnp.asarray(sizes, jnp.int32))

    sizes = jnp.where(number % 4 == 0, named(crowded, number // 4), named(ordinary, number - number // 4 - 1))
    mixed = jax.random.permutation(jax.random.fold_in(own, 3), amount)
    source_of, receiver = mixed[0:amount // 2 * 2:2], mixed[1:amount // 2 * 2:2]
    margin = jnp.minimum(sizes[source_of] - 1, bound - sizes[receiver]) // 2
    margin = jnp.where((source_of == ranking[0]) | (receiver == ranking[0]) | (sizes[receiver] == 0), 0, jnp.maximum(margin, 0))
    moved = jax.random.randint(jax.random.fold_in(own, 4), (amount // 2,), 0, 1 << 20) % (margin + 1)
    sizes = sizes.at[source_of].add(-moved).at[receiver].add(moved)
    items = jnp.searchsorted(jnp.cumsum(sizes), jnp.arange(rows * top), side="right").astype(jnp.int32)
    grid = items.reshape(top, rows).T
    grid = grid[jax.random.permutation(jax.random.fold_in(own, 1), rows)]
    rotation = jax.random.randint(jax.random.fold_in(own, 2), (rows, 1), 0, top)
    return jnp.take_along_axis(grid, (jnp.arange(top)[None, :] + rotation) % top, axis=1)


def portions_of(number_of, total, limit, slope, full):
    weights = [(1 << 20) // math.isqrt(standing ** slope) + 1 for standing in range(1, number_of + 1)]
    largest = limit if full else min(limit, max(-(-total // number_of), total * weights[0] // sum(weights)))
    least = 1 if total - largest >= number_of - 1 else 0
    counts, rest = [largest] + [least] * (number_of - 1), total - largest - least * (number_of - 1)
    while rest > 0:
        candidates = [i for i in range(1, number_of) if counts[i] < largest] or [i for i in range(1, number_of) if counts[i] < limit]
        pool, remaining = sum([weights[i] for i in candidates]), rest
        for i in candidates:
            addition = min(limit - counts[i], max(1, remaining * weights[i] // pool), rest)
            counts[i] = counts[i] + addition
            rest = rest - addition
    return np.array(counts)


def gaussian(key, extent, deviation, reach, split=(), kind=jnp.bfloat16):
    level = level_of(key, extent, split, -0.22, 0.18) if split else 1.0
    entries = jax.random.normal(key, extent, jnp.float32) * deviation * level
    return jnp.minimum(jnp.maximum(entries, -reach), reach).astype(kind)


def gaussian_with(own_key, shape, deviation, limit, split, heavy, held_as=jnp.bfloat16):
    entries = deviation * jax.random.normal(own_key, shape, jnp.float32)
    if split:
        entries = entries * level_of(own_key, shape, split, -0.22, 0.18)
    return jnp.clip(raised(entries, jax.random.fold_in(own_key, 3), *heavy), -limit, limit).astype(held_as)


def setup_inputs(seed: int = 0) -> dict:
    keys = jax.random.split(jax.random.key(seed), 22)
    tokens = gaussian(keys[0], (BATCH, D), 1.0, 6.0, ((0, 8),))
    attn_gain = jnp.clip(1.0 + 0.18 * jax.random.normal(keys[1], (D,), jnp.float32), 0.1, 1.9)
    query_weight = gaussian(keys[2], (D, H * DH), D ** -0.5, 0.125, ((0, 8), (1, 4)))
    key_weight = gaussian(keys[3], (D, H * DH), D ** -0.5, 0.125, ((0, 8), (1, 4)))
    value_weight = gaussian(keys[4], (D, H * DH), D ** -0.5, 0.125, ((0, 8), (1, 4)))
    query_gain = jnp.clip(1.0 + 0.18 * jax.random.normal(keys[5], (DH,), jnp.float32), 0.1, 1.9)
    stick_bias = jnp.clip(-7.0 + 4.5 * jax.random.uniform(keys[6], (H,), jnp.float32) ** level_of(keys[6], (H,), ((0, 4),), -0.2, 0.2), -7.0, -2.5)
    key_cache = gaussian(keys[7], (BATCH, H, L, DH), 1.0, 6.0, ((0, 8), (1, 4)))
    value_cache = gaussian(keys[8], (BATCH, H, L, DH), 1.0, 6.0, ((0, 8), (1, 4)))
    lengths = draw_lengths(jax.random.fold_in(keys[21], 71), 0)
    out_weight = gaussian(keys[10], (H * DH, D), (H * DH // 16) ** -0.5, 0.375, ((0, 4),))
    mix_gain = jnp.clip(1.0 + 0.18 * jax.random.normal(keys[11], (D,), jnp.float32), 0.1, 1.9)
    route_ids_keys = jax.random.split(jax.random.fold_in(keys[12], 1), BATCH // SEQS)
    route_ids_turns = jax.random.permutation(jax.random.fold_in(keys[12], 3), BATCH // SEQS)
    route_ids = jax.vmap(lambda own, number: routed_block(jax.random.fold_in(keys[12], 2), own, number, SEQS, E, TOP, CAP, 2))(route_ids_keys, route_ids_turns).reshape((BATCH, TOP))
    route_weights = jnp.clip(0.2 + 0.8 * jax.random.uniform(keys[13], (BATCH, TOP), jnp.float32) ** level_of(keys[13], (BATCH, TOP), ((0, 8),), -0.2, 0.2), 0.2, 1.0)
    expert_gate = gaussian(keys[14], (E, D, FF_E), D ** -0.5, 0.125, ((0, 8), (2, 4)))
    expert_up = gaussian(keys[15], (E, D, FF_E), D ** -0.5, 0.125, ((0, 8), (2, 4)))
    expert_down = gaussian_with(keys[16], (E, FF_E, D), FF_E ** -0.5, 0.15625, ((0, 8), (1, 4)), (1, 2, 4, 2.0))
    side_gate = gaussian(keys[17], (D, SH), D ** -0.5, 0.125, ((1, 4),))
    side_up = gaussian(keys[18], (D, SH), D ** -0.5, 0.125, ((1, 4),))
    side_down = gaussian_with(keys[19], (SH, D), SH ** -0.5, 0.25, ((0, 4),), (0, 1, 4, 2.0))
    branch_gate = gaussian(keys[20], (D,), D ** -0.5, 0.125, (), jnp.float32)
    return dict(tokens=tokens, attn_gain=attn_gain, query_weight=query_weight, key_weight=key_weight, value_weight=value_weight, query_gain=query_gain, stick_bias=stick_bias, key_cache=key_cache, value_cache=value_cache, lengths=lengths, out_weight=out_weight, mix_gain=mix_gain, route_ids=route_ids, route_weights=route_weights, expert_gate=expert_gate, expert_up=expert_up, expert_down=expert_down, side_gate=side_gate, side_up=side_up, side_down=side_down, branch_gate=branch_gate)


epsilon = 1e-06

def rms_scale(values, scale_gain):
    mean_square = lax.optimization_barrier(jnp.mean(values * values, axis=-1, keepdims=True))
    return values * lax.rsqrt(mean_square + epsilon) * scale_gain

def expert_apply(bundle):
    slot_rows, gate_w, up_w, down_w = bundle
    gate_pre = jnp.dot(slot_rows, gate_w, preferred_element_type=jnp.float32)
    up_pre = jnp.dot(slot_rows, up_w, preferred_element_type=jnp.float32)
    hidden = (jax.nn.silu(gate_pre) * up_pre).astype(jnp.bfloat16)
    return jnp.dot(hidden, down_w, preferred_element_type=jnp.float32).astype(jnp.bfloat16)

def reference(tokens, attn_gain, query_weight, key_weight, value_weight, query_gain, stick_bias, key_cache, value_cache, lengths, out_weight, mix_gain, route_ids, route_weights, expert_gate, expert_up, expert_down, side_gate, side_up, side_down, branch_gate):
    stream = tokens.astype(jnp.float32)
    normed = rms_scale(stream, attn_gain).astype(jnp.bfloat16)
    query_rows = jnp.dot(normed, query_weight, preferred_element_type=jnp.float32).astype(jnp.bfloat16)
    fresh_keys = jnp.dot(normed, key_weight, preferred_element_type=jnp.float32).astype(jnp.bfloat16)
    new_values = jnp.dot(normed, value_weight, preferred_element_type=jnp.float32).astype(jnp.bfloat16)
    batch_count = tokens.shape[0]
    new_keys = rms_scale(fresh_keys.astype(jnp.float32).reshape(batch_count, H, DH), 1.0)
    new_keys = new_keys.astype(jnp.bfloat16).reshape(batch_count, H * DH)
    query_heads = rms_scale(query_rows.astype(jnp.float32).reshape(batch_count, H, DH), query_gain)
    query_heads = query_heads.astype(jnp.bfloat16)

    def attend_one(bundle):
        query_row, key_rows, value_rows, length = bundle
        scores = jnp.einsum('hd,hld->hl', query_row.astype(jnp.float32), key_rows.astype(jnp.float32))
        scores = scores * DH ** (-0.5) + stick_bias[:, None]
        positions = jnp.arange(L, dtype=jnp.int32)
        visible = positions[None, :] < length
        log_rest = jnp.where(visible, jax.nn.log_sigmoid(-scores), 0.0)
        log_between = lax.cumsum(log_rest, axis=1, reverse=True) - log_rest
        stick = jnp.where(visible, jnp.exp(jax.nn.log_sigmoid(scores) + log_between), 0.0).astype(jnp.bfloat16)
        attended = jnp.einsum('hl,hld->hd', stick.astype(jnp.float32), value_rows.astype(jnp.float32))
        return attended.astype(jnp.bfloat16).reshape(H * DH)
    attended = lax.map(attend_one, (query_heads, key_cache, value_cache, lengths))
    attn_proj = jnp.dot(attended, out_weight, preferred_element_type=jnp.float32)
    middle = (stream + attn_proj).astype(jnp.bfloat16)
    normed_mix = rms_scale(middle.astype(jnp.float32), mix_gain).astype(jnp.bfloat16)
    flat_ids = route_ids.reshape(N_EP, SEQS * TOP)
    onehot = (flat_ids[:, :, None] == jnp.arange(E, dtype=jnp.int32)[None, None, :]).astype(jnp.int32)
    before = jnp.cumsum(onehot, axis=1) - onehot
    slot_index = lax.optimization_barrier(jnp.sum(before * onehot, axis=2))
    sources = jnp.arange(N_EP, dtype=jnp.int32)[:, None]
    target = ((flat_ids * N_EP + sources) * CAP + slot_index).reshape(-1).astype(jnp.int32)
    slot_table = jnp.zeros((E * N_EP * CAP,), jnp.int32).at[target].set(jnp.arange(BATCH * TOP, dtype=jnp.int32))
    slot_rows = normed_mix[slot_table // TOP].reshape(E, N_EP * CAP, D)
    expert_outs = lax.map(expert_apply, (slot_rows, expert_gate, expert_up, expert_down))
    route_out = expert_outs.reshape(E * N_EP * CAP, D)[target].astype(jnp.float32).reshape(BATCH, TOP, D)
    routed = lax.optimization_barrier(jnp.sum(route_weights[:, :, None] * route_out, axis=1))
    side_gate_pre = jnp.dot(normed_mix, side_gate, preferred_element_type=jnp.float32)
    side_up_pre = jnp.dot(normed_mix, side_up, preferred_element_type=jnp.float32)
    side_hidden = (jax.nn.silu(side_gate_pre) * side_up_pre).astype(jnp.bfloat16)
    side_out = jnp.dot(side_hidden, side_down, preferred_element_type=jnp.float32)
    switch = jax.nn.sigmoid(lax.optimization_barrier(jnp.sum(normed_mix.astype(jnp.float32) * branch_gate, axis=1, keepdims=True)))
    mixed = (middle.astype(jnp.float32) + routed + switch * side_out).astype(jnp.bfloat16)
    return (mixed, new_keys, new_values)
```

```python
import jax
import jax.numpy as jnp
from jax import lax
from jax.experimental import pallas as pl
from jax.experimental.pallas import tpu as pltpu
from jax.sharding import PartitionSpec as P

DH = 128


epsilon = 1e-06


def rms_scale(values, scale_gain):
    mean_square = jnp.mean(values * values, axis=-1, keepdims=True)
    return values * lax.rsqrt(mean_square + epsilon) * scale_gain


def body(
    tokens,
    attn_gain,
    query_weight,
    key_weight,
    value_weight,
    query_gain,
    stick_bias,
    key_cache,
    value_cache,
    lengths,
    out_weight,
    mix_gain,
    route_ids,
    route_weights,
    expert_gate,
    expert_up,
    expert_down,
    side_gate,
    side_up,
    side_down,
    branch_gate,
):
    seq_count, model_width = tokens.shape
    head_cols = query_weight.shape[1]
    heads_local = key_cache.shape[1]
    cache_slots = key_cache.shape[2]
    stream = tokens.astype(jnp.float32)
    normed = rms_scale(stream, attn_gain).astype(jnp.bfloat16)
    stacked = jnp.concatenate([query_weight, key_weight, value_weight], axis=1)
    columns = lax.all_to_all(normed, "ep", split_axis=1, concat_axis=0, tiled=True)
    picked = columns
    projected = lax.psum_scatter(
        jnp.dot(picked, stacked, preferred_element_type=jnp.float32),
        "ep",
        scatter_dimension=0,
        tiled=True,
    )
    query_rows = projected[:, :head_cols].astype(jnp.bfloat16)
    fresh_keys = projected[:, head_cols : 2 * head_cols].astype(jnp.bfloat16)
    new_values = projected[:, 2 * head_cols :].astype(jnp.bfloat16)
    new_keys = rms_scale(fresh_keys.astype(jnp.float32).reshape(seq_count, heads_local, DH), 1.0)
    new_keys = new_keys.astype(jnp.bfloat16).reshape(seq_count, head_cols)
    query_heads = rms_scale(
        query_rows.astype(jnp.float32).reshape(seq_count, heads_local, DH), query_gain
    )
    query_heads = query_heads.astype(jnp.bfloat16)
    scores = jnp.einsum("shd,shld->shl", query_heads, key_cache, preferred_element_type=jnp.float32)
    scores = scores * DH ** (-0.5) + stick_bias[None, :, None]
    positions = jnp.arange(cache_slots, dtype=jnp.int32)
    visible = positions[None, None, :] < lengths[:, None, None]
    log_rest = jnp.where(visible, jax.nn.log_sigmoid(-scores), 0.0)
    log_between = lax.cumsum(log_rest, axis=2, reverse=True) - log_rest
    stick = jnp.where(visible, jnp.exp(jax.nn.log_sigmoid(scores) + log_between), 0.0).astype(
        jnp.bfloat16
    )
    attended = jnp.einsum("shl,shld->shd", stick, value_cache, preferred_element_type=jnp.float32)
    attended = attended.astype(jnp.bfloat16).reshape(seq_count, head_cols)
    attn_proj = lax.psum(
        jnp.dot(attended, out_weight, preferred_element_type=jnp.float32).astype(jnp.bfloat16), "tp"
    ).astype(jnp.float32)
    middle = (stream + attn_proj).astype(jnp.bfloat16)
    normed_mix = rms_scale(middle.astype(jnp.float32), mix_gain).astype(jnp.bfloat16)
    side_gate_pre = jnp.dot(normed_mix, side_gate, preferred_element_type=jnp.float32)
    side_up_pre = jnp.dot(normed_mix, side_up, preferred_element_type=jnp.float32)
    side_hidden = (jax.nn.silu(side_gate_pre) * side_up_pre).astype(jnp.bfloat16)
    side_term = jnp.dot(side_hidden, side_down, preferred_element_type=jnp.float32)
    switch = jax.nn.sigmoid(
        jnp.sum(normed_mix.astype(jnp.float32) * branch_gate, axis=1, keepdims=True)
    )
    experts = lax.axis_size("ep")
    top_count = route_ids.shape[1]
    capacity = max(2, 2 * top_count * seq_count // experts)
    flat_ids = route_ids.reshape(-1)
    onehot = (flat_ids[:, None] == jnp.arange(experts, dtype=jnp.int32)[None, :]).astype(jnp.int32)
    before = jnp.cumsum(onehot, axis=0) - onehot
    slot_index = jnp.sum(before * onehot, axis=1)
    target = flat_ids * capacity + slot_index
    route_map = (
        target[:, None] == jnp.arange(experts * capacity, dtype=jnp.int32)[None, :]
    ).astype(jnp.bfloat16)
    dispatch = jnp.sum(route_map.reshape(seq_count, top_count, experts * capacity), axis=1).T
    outbox = jnp.dot(dispatch, normed_mix, preferred_element_type=jnp.float32).astype(jnp.bfloat16)
    outbox = outbox.reshape(experts, capacity, model_width)
    col_width = model_width // lax.axis_size("tp")
    col_offset = lax.axis_index("tp") * col_width
    arrived = lax.all_to_all(outbox, "ep", split_axis=0, concat_axis=0, tiled=True)
    slot_rows = arrived.reshape(experts * capacity, model_width)
    gate_pre = jnp.dot(slot_rows, expert_gate[0], preferred_element_type=jnp.float32)
    up_pre = jnp.dot(slot_rows, expert_up[0], preferred_element_type=jnp.float32)
    hidden = (jax.nn.silu(gate_pre) * up_pre).astype(jnp.bfloat16)
    expert_term = jnp.dot(hidden, expert_down[0], preferred_element_type=jnp.float32)
    expert_part, side_part = (
        lax.psum_scatter(
            expert_term.astype(jnp.bfloat16), "tp", scatter_dimension=1, tiled=True
        ).astype(jnp.float32),
        lax.psum_scatter(
            side_term.astype(jnp.bfloat16), "tp", scatter_dimension=1, tiled=True
        ).astype(jnp.float32),
    )
    returned = lax.all_to_all(
        expert_part.astype(jnp.bfloat16).reshape(experts, capacity, col_width),
        "ep",
        split_axis=0,
        concat_axis=0,
        tiled=True,
    )
    picked = jnp.dot(
        route_map,
        returned.reshape(experts * capacity, col_width),
        preferred_element_type=jnp.float32,
    )
    routed = jnp.sum(
        route_weights[:, :, None] * picked.reshape(seq_count, top_count, col_width), axis=1
    )
    middle_cols = lax.dynamic_slice_in_dim(middle, col_offset, col_width, 1).astype(jnp.float32)
    mixed = (middle_cols + routed + switch * side_part).astype(jnp.bfloat16)
    return (mixed, new_keys, new_values)


MESH = pl.DeviceIdType.MESH
F32 = jnp.float32
BF16 = jnp.bfloat16


def softplus(values):
    return jnp.maximum(values, 0.0) + jnp.log1p(jnp.exp(-jnp.abs(values)))


def silu(values):
    return values / (1.0 + jnp.exp(-values))


def as_columns(rows):
    count = rows.shape[1]
    own = lax.broadcasted_iota(jnp.int32, (count, count), 0) == lax.broadcasted_iota(
        jnp.int32, (count, count), 1
    )
    rows = rows.astype(F32)
    return [
        jnp.sum(jnp.where(own, rows[i : i + 1], 0.0), axis=1, keepdims=True)
        for i in range(rows.shape[0])
    ]


class Phases:
    def __init__(self):
        self.scope = None

    def __call__(self, name):
        if self.scope is not None:
            self.scope.__exit__(None, None, None)
        self.scope = jax.named_scope(name) if name else None
        if self.scope is not None:
            self.scope.__enter__()


def stack_rows(buffer):
    return jnp.concatenate([buffer[i].astype(F32) for i in range(buffer.shape[0])], axis=0)


def layer_kernel(
    n,
    m,
    tokens_hbm,
    attn_gain_hbm,
    query_gain_hbm,
    bias_hbm,
    lengths_hbm,
    mix_gain_hbm,
    ids_hbm,
    weights_hbm,
    branch_hbm,
    wq_hbm,
    wk_hbm,
    wv_hbm,
    key_hbm,
    value_hbm,
    out_hbm,
    gate_hbm,
    up_hbm,
    down_hbm,
    side_gate_hbm,
    side_up_hbm,
    side_down_hbm,
    mixed_ref,
    new_keys_ref,
    new_values_ref,
    tokens_ref,
    rows_ref,
    query_gain_ref,
    bias_ref,
    lengths_ref,
    ids_ref,
    weights_ref,
    proj_w,
    keys,
    turned,
    values,
    out_w,
    expert_w,
    down_w,
    side_w,
    side_down_w,
    col_send,
    col_recv,
    query_send,
    query_recv,
    proj_send,
    proj_recv,
    reduce_buf,
    mid_cols,
    mix_send,
    mix_recv,
    slot_rows,
    slot_cols,
    side_cols,
    side_send,
    side_recv,
    back_send,
    back_recv,
    load_sem,
    send_sem,
    recv_sem,
):
    ep = lax.axis_index("ep")
    tp = lax.axis_index("tp")
    seqs, width = tokens_ref.shape
    heads, dh, slots = turned.shape[0], turned.shape[2], turned.shape[3]
    cols = width // n
    out_cols = width // m
    parts = reduce_buf.shape[0]
    part_cols = width // parts

    phase_name = Phases()
    phase_name("greet")
    barrier = pltpu.get_barrier_semaphore()
    for d in range(1, n):
        pl.semaphore_signal(barrier, inc=1, device_id=(lax.rem(ep + d, n), tp), device_id_type=MESH)
    for d in range(1, m):
        pl.semaphore_signal(barrier, inc=1, device_id=(ep, lax.rem(tp + d, m)), device_id_type=MESH)

    def load(k, whole, *pairs, priority=1):
        for src, dst in pairs:
            pltpu.make_async_copy(src, dst, load_sem.at[k]).start(priority=priority)
        return pltpu.make_async_copy(whole, whole, load_sem.at[k])

    tokens_load = load(0, tokens_ref, (tokens_hbm, tokens_ref), priority=0)
    gains = (attn_gain_hbm, mix_gain_hbm, branch_hbm)
    rows_load = load(1, rows_ref, *((x, rows_ref.at[i]) for i, x in enumerate(gains)), priority=0)
    small = (
        (ids_hbm, ids_ref),
        (weights_hbm, weights_ref),
        (query_gain_hbm, query_gain_ref),
        (bias_hbm, bias_ref),
        (lengths_hbm, lengths_ref),
    )
    small_loads = [load(2 + i, x[1], x, priority=0) for i, x in enumerate(small)]
    proj_load = load(
        7,
        proj_w,
        *((w, proj_w.at[i]) for i, w in enumerate((wq_hbm, wk_hbm, wv_hbm))),
        priority=0,
    )
    key_load = load(8, keys, *((key_hbm.at[i], keys.at[i]) for i in range(seqs)))
    value_load = load(9, values, *((value_hbm.at[i], values.at[:, i]) for i in range(seqs)))

    def remote(sem, src, dst, target, arrival=None):
        copy = pltpu.make_async_remote_copy(
            src_ref=src,
            dst_ref=dst,
            send_sem=send_sem.at[sem],
            recv_sem=recv_sem.at[sem if arrival is None else arrival],
            device_id=target,
            device_id_type=MESH,
        )
        copy.start()

    def sent(sem, whole):
        pltpu.make_async_copy(whole, whole, send_sem.at[sem]).wait()

    def arrived(sem, whole):
        pltpu.make_async_copy(whole, whole, recv_sem.at[sem]).wait()

    def ep_scatter(sem, send, recv, arrival=None):
        for d in range(1, n):
            j = lax.rem(ep + d, n)
            remote(sem, send.at[j], recv.at[ep], (j, tp), arrival)

    others = pl.ds(0, n - 1)
    fellows = pl.ds(0, m - 1)
    s_col, s_query, s_proj, s_reduce, s_mix, s_side, s_back, s_near = range(8)
    r_query, r_reduce, r_mix = 8, 10, 10 + parts

    tokens_load.wait()
    rows_load.wait()
    attn_gain, mix_gain, branch_gate = (rows_ref[i] for i in range(3))
    stream = tokens_ref[...].astype(F32)
    normed = rms_scale(stream, attn_gain)
    for j in range(n):
        col_send[j] = normed[:, j * cols : (j + 1) * cols].astype(BF16)
    col_recv[ep] = col_send[ep]
    phase_name("barrier")
    pl.semaphore_wait(barrier, (n - 1) + (m - 1))
    phase_name("col_send")
    ep_scatter(s_col, col_send, col_recv)

    for copy in small_loads:
        copy.wait()
    later = lax.broadcasted_iota(jnp.int32, (slots, slots), 0) > lax.broadcasted_iota(
        jnp.int32, (slots, slots), 1
    )
    later = jnp.where(later, 1.0, 0.0).astype(BF16)
    capacity = mix_send.shape[2]
    lane_expert = lax.broadcasted_iota(jnp.int32, (seqs, n), 1).astype(F32)
    lane_slot = lax.broadcasted_iota(jnp.int32, (seqs, n * capacity), 1).astype(F32)
    row_slot = lax.broadcasted_iota(jnp.int32, (n * capacity, seqs), 0).astype(F32)
    first = lax.broadcasted_iota(jnp.int32, (seqs, seqs), 0)
    second = lax.broadcasted_iota(jnp.int32, (seqs, seqs), 1)
    weights = as_columns(weights_ref[...])
    ids = as_columns(ids_ref[...])
    named = [jnp.where(lane_expert == i, 1.0, 0.0) for i in ids]
    before = jnp.dot(
        jnp.where(second < first, 1.0, 0.0).astype(BF16),
        sum(named).astype(BF16),
        preferred_element_type=F32,
    )
    targets = [
        i * float(capacity) + jnp.sum(before * x, axis=1, keepdims=True) for i, x in zip(ids, named)
    ]
    route_map = jnp.concatenate(
        [jnp.where(lane_slot == t, 1.0, 0.0) for t in targets], axis=0
    ).astype(BF16)
    dispatch = sum(
        jnp.where(
            row_slot == jnp.sum(jnp.where(first == second, t, 0.0), axis=0, keepdims=True), 1.0, 0.0
        )
        for t in targets
    ).astype(BF16)
    proj_load.wait()
    phase_name("col_wait")
    arrived(s_col, col_recv.at[others])
    phase_name("project")
    picked = stack_rows(col_recv).astype(BF16)

    half = query_send.shape[3]
    for g in range(2):
        part = jnp.dot(
            picked, proj_w[0, :, g * half : (g + 1) * half], preferred_element_type=F32
        )
        for j in range(n):
            query_send[g, j] = part[j * seqs : (j + 1) * seqs].astype(BF16)
        query_recv[g, ep] = query_send[g, ep]
        ep_scatter(s_query, query_send.at[g], query_recv.at[g], r_query + g)
    phase_name("turn")
    out_load = load(10, out_w, (out_hbm, out_w))
    side_load = load(11, side_w, (side_gate_hbm, side_w.at[0]), (side_up_hbm, side_w.at[1]))
    side_down_load = load(12, side_down_w, (side_down_hbm, side_down_w))
    expert_load = load(13, expert_w, (gate_hbm.at[0], expert_w.at[0]), (up_hbm.at[0], expert_w.at[1]))
    down_load = load(14, down_w, (down_hbm.at[0], down_w))
    for i in (1, 2):
        part = jnp.dot(picked, proj_w[i], preferred_element_type=F32)
        for j in range(n):
            proj_send[i - 1, j] = part[j * seqs : (j + 1) * seqs].astype(BF16)
        proj_recv[i - 1, ep] = proj_send[i - 1, ep]
    key_load.wait()
    for s in range(seqs):
        for h in range(heads):
            turned[h, s] = keys[s, h].T
    value_load.wait()

    def collect(recv):
        total = recv[0].astype(F32)
        for j in range(1, n):
            total = total + recv[j].astype(F32)
        return total.astype(BF16).astype(F32)

    query_row = lax.broadcasted_iota(jnp.int32, (seqs, dh), 0)
    slot_row = lax.broadcasted_iota(jnp.int32, (seqs, slots), 0)
    position = lax.broadcasted_iota(jnp.int32, (seqs, slots), 1)
    lengths = as_columns(lengths_ref[...])[0].astype(jnp.int32)
    visible = position < lengths
    scale = dh ** (-0.5)
    some = half // dh
    score_rows, rest_rows = [], []
    for g in range(2):
        phase_name("query_wait")
        arrived(r_query + g, query_recv.at[g, others])
        phase_name("scores")
        query = collect(query_recv.at[g])
        if g == 0:
            for i in range(2):
                ep_scatter(s_proj, proj_send.at[i], proj_recv.at[i])
        for k in range(some):
            h = g * some + k
            q = rms_scale(query[:, k * dh : (k + 1) * dh], query_gain_ref[...])
            spread = jnp.concatenate(
                [jnp.where(query_row == s, q, 0.0).astype(BF16) for s in range(seqs)], axis=1
            )
            score = jnp.dot(
                spread, turned[h].reshape(seqs * dh, slots), preferred_element_type=F32
            )
            score = score * scale + bias_ref[0:1, h : h + 1]
            full = -softplus(score)
            score_rows.append(score + full)
            rest_rows.append(jnp.where(visible, full, 0.0))
    rest = jnp.concatenate(rest_rows, axis=0)
    high = rest.astype(BF16)
    left = rest - high.astype(F32)
    middle_part = left.astype(BF16)
    low = (left - middle_part.astype(F32)).astype(BF16)
    pieces = jnp.dot(
        jnp.concatenate([high, middle_part, low], axis=0), later, preferred_element_type=F32
    )
    count = seqs * heads
    between = pieces[:count] + pieces[count : 2 * count] + pieces[2 * count :]
    attended = []
    for h in range(heads):
        stick = jnp.where(
            visible, jnp.exp(score_rows[h] + between[h * seqs : (h + 1) * seqs]), 0.0
        )
        spread = jnp.concatenate(
            [jnp.where(slot_row == s, stick, 0.0).astype(BF16) for s in range(seqs)], axis=1
        )
        attended.append(
            jnp.dot(spread, values[h].reshape(seqs * slots, dh), preferred_element_type=F32)
        )
    attended = jnp.concatenate(attended, axis=1).astype(BF16)
    phase_name("out_proj")
    out_load.wait()
    for t in range(parts):
        reduce_buf[t, tp] = jnp.dot(
            attended, out_w[:, t * part_cols : (t + 1) * part_cols], preferred_element_type=F32
        ).astype(BF16)
        for d in range(1, m):
            own = reduce_buf.at[t, tp]
            remote(s_reduce, own, own, (ep, lax.rem(tp + d, m)), r_reduce + t)

    middle = []
    for t in range(parts):
        phase_name("reduce_wait")
        arrived(r_reduce + t, reduce_buf.at[t, fellows])
        phase_name("mix")
        total = sum(reduce_buf[t, i].astype(F32) for i in range(m))
        part = (stream[:, t * part_cols : (t + 1) * part_cols] + total).astype(BF16)
        outbox = jnp.dot(dispatch, part, preferred_element_type=F32)
        for j in range(n):
            mix_send[t, j] = outbox[j * capacity : (j + 1) * capacity].astype(BF16)
        mix_recv[t, ep] = mix_send[t, ep]
        ep_scatter(s_mix, mix_send.at[t], mix_recv.at[t], r_mix + t)
        middle.append(part.astype(F32))
    middle = jnp.concatenate(middle, axis=1)
    for t in range(m):
        mid_cols[t] = middle[:, t * out_cols : (t + 1) * out_cols]

    phase_name("side")
    normed_mix = rms_scale(middle, mix_gain).astype(BF16)
    side_load.wait()
    side_down_load.wait()
    side_hidden = silu(
        jnp.dot(normed_mix, side_w[0], preferred_element_type=F32)
    ) * jnp.dot(normed_mix, side_w[1], preferred_element_type=F32)
    side_term = jnp.dot(side_hidden.astype(BF16), side_down_w[...], preferred_element_type=F32)
    switch = jnp.sum(normed_mix.astype(F32) * branch_gate, axis=1, keepdims=True)
    switch = 1.0 / (1.0 + jnp.exp(-switch))
    for t in range(m):
        side_cols[t] = switch * side_term[:, t * out_cols : (t + 1) * out_cols]
    for d in range(1, m):
        t = lax.rem(tp + d, m)
        side_send[d - 1] = side_cols[t].astype(BF16)
        remote(s_side, side_send.at[d - 1], side_recv.at[d - 1], (ep, t))

    phase_name("new_keys")
    arrived(s_proj, proj_recv.at[:, others])
    key_rows = collect(proj_recv.at[0])
    for h in range(heads):
        part = slice(h * dh, (h + 1) * dh)
        new_keys_ref[:, part] = rms_scale(key_rows[:, part], 1.0).astype(BF16)
    new_values_ref[...] = collect(proj_recv.at[1]).astype(BF16)
    expert_load.wait()
    down_load.wait()
    sent(s_col, col_send.at[others])
    sent(s_query, query_send.at[:, others])
    sent(s_proj, proj_send.at[:, others])
    sent(s_reduce, reduce_buf.at[:, fellows])

    gate_pre = up_pre = squares = None
    for t in range(parts):
        phase_name("rows_wait")
        arrived(r_mix + t, mix_recv.at[t, others])
        phase_name("expert")
        for j in range(n):
            slot_rows[t, j * capacity : (j + 1) * capacity, :] = mix_recv[t, j].astype(F32)
        span = slice(t * part_cols, (t + 1) * part_cols)
        rows = slot_rows[t]
        square = jnp.sum(rows * rows, axis=1, keepdims=True)
        rows = (rows * mix_gain[:, span]).astype(BF16)
        gate_part = jnp.dot(rows, expert_w[0, span, :], preferred_element_type=F32)
        up_part = jnp.dot(rows, expert_w[1, span, :], preferred_element_type=F32)
        gate_pre = gate_part if t == 0 else gate_pre + gate_part
        up_pre = up_part if t == 0 else up_pre + up_part
        squares = square if t == 0 else squares + square
    factor = lax.rsqrt(squares / width + epsilon)
    hidden = (silu(gate_pre * factor) * (up_pre * factor)).astype(BF16)
    for t in range(m):
        expert_term = jnp.dot(
            hidden, down_w[:, t * out_cols : (t + 1) * out_cols], preferred_element_type=F32
        )
        for j in range(n):
            back_send[t, j] = expert_term[j * capacity : (j + 1) * capacity].astype(BF16)
        for k in range(n - 1):
            j = k + (k - ep + n) // n
            remote(s_back, back_send.at[t, j], back_recv.at[tp, ep], (j, t))
    for d in range(1, m):
        t = lax.rem(tp + d, m)
        remote(s_near, back_send.at[t, ep], back_recv.at[tp, ep], (ep, t))
    back_recv[tp, ep] = back_send[tp, ep]
    phase_name("side_wait")
    result = mid_cols[tp] + side_cols[tp]
    arrived(s_side, side_recv.at[...])
    for d in range(1, m):
        result = result + side_recv[d - 1].astype(F32)
    sent(s_mix, mix_send.at[:, others])
    sent(s_side, side_send.at[...])
    phase_name("back_wait")
    arrived(s_near, back_recv.at[fellows, 0])
    arrived(s_back, back_recv.at[:, others])
    phase_name("combine")
    for j in range(n):
        slot_cols[j * capacity : (j + 1) * capacity, :] = sum(
            back_recv[i, j].astype(F32) for i in range(m)
        )
    chosen = jnp.dot(route_map, slot_cols[...].astype(BF16), preferred_element_type=F32)
    for k, w in enumerate(weights):
        result = result + w * chosen[k * seqs : (k + 1) * seqs]
    mixed_ref[...] = result.astype(BF16)
    phase_name("drain")
    sent(s_near, back_send.at[fellows, 0])
    sent(s_back, back_send.at[:, others])
    phase_name(None)


def hand_on(count, *refs):
    sources, targets, sem = refs[:count], refs[count : 2 * count], refs[-1]
    copies = [
        pltpu.make_async_copy(src, dst, sem.at[i])
        for i, (src, dst) in enumerate(zip(sources, targets))
    ]
    for copy in copies:
        copy.start()
    for copy in copies:
        copy.wait()


def fused(n, m, *args):
    (
        tokens,
        attn_gain,
        query_weight,
        key_weight,
        value_weight,
        query_gain,
        stick_bias,
        key_cache,
        value_cache,
        lengths,
        out_weight,
        mix_gain,
        route_ids,
        route_weights,
        expert_gate,
        expert_up,
        expert_down,
        side_gate,
        side_up,
        side_down,
        branch_gate,
    ) = args
    seqs, width = tokens.shape
    _, heads, slots, dh = key_cache.shape
    head_cols = query_weight.shape[1]
    out_cols = width // m
    capacity = max(2, 2 * route_ids.shape[1] * seqs // n)
    parts = 2
    vmem = pl.BlockSpec(memory_space=pltpu.VMEM)
    hbm = pl.BlockSpec(memory_space=pl.ANY)
    dma = pltpu.SemaphoreType.DMA

    def scratch(*shape, dtype=BF16):
        return pltpu.VMEM(shape, dtype)

    small = (
        tokens,
        attn_gain.reshape(1, width),
        query_gain.reshape(1, dh),
        stick_bias.reshape(1, heads),
        lengths.reshape(1, seqs),
        mix_gain.reshape(1, width),
        route_ids.T,
        route_weights.T,
        branch_gate.reshape(1, width),
    )
    shapes = ((seqs, out_cols), (seqs, head_cols), (seqs, head_cols))
    outs = pl.pallas_call(
        lambda *refs: layer_kernel(n, m, *refs),
        out_shape=tuple(pltpu.VMEM(shape, BF16) for shape in shapes),
        in_specs=[hbm] * 21,
        out_specs=(vmem, vmem, vmem),
        scratch_shapes=[
            scratch(seqs, width),
            scratch(3, 1, width, dtype=F32),
            *(scratch(*x.shape, dtype=x.dtype) for x in (*small[2:5], *small[6:8])),
            scratch(3, *query_weight.shape),
            scratch(*key_cache.shape),
            scratch(heads, seqs, dh, slots),
            scratch(heads, seqs, slots, dh),
            scratch(*out_weight.shape),
            scratch(2, *expert_gate.shape[1:]),
            scratch(*expert_down.shape[1:]),
            scratch(2, *side_gate.shape),
            scratch(*side_down.shape),
            scratch(n, seqs, width // n),
            scratch(n, seqs, width // n),
            scratch(2, n, seqs, head_cols // 2),
            scratch(2, n, seqs, head_cols // 2),
            scratch(2, n, seqs, head_cols),
            scratch(2, n, seqs, head_cols),
            scratch(parts, m, seqs, width // parts),
            scratch(m, seqs, out_cols, dtype=F32),
            scratch(parts, n, capacity, width // parts),
            scratch(parts, n, capacity, width // parts),
            scratch(parts, n * capacity, width // parts, dtype=F32),
            scratch(n * capacity, out_cols, dtype=F32),
            scratch(m, seqs, out_cols, dtype=F32),
            scratch(m - 1, seqs, out_cols),
            scratch(m - 1, seqs, out_cols),
            scratch(m, n, capacity, out_cols),
            scratch(m, n, capacity, out_cols),
            dma((15,)),
            dma((8,)),
            dma((10 + 2 * parts,)),
        ],
        compiler_params=pltpu.CompilerParams(
            collective_id=0, has_side_effects=True, vmem_limit_bytes=60 * 1024 * 1024
        ),
        name="layer",
    )(
        *small,
        query_weight,
        key_weight,
        value_weight,
        key_cache,
        value_cache,
        out_weight,
        expert_gate,
        expert_up,
        expert_down,
        side_gate,
        side_up,
        side_down,
    )
    return pl.pallas_call(
        lambda *refs: hand_on(len(shapes), *refs),
        out_shape=tuple(jax.ShapeDtypeStruct(shape, BF16) for shape in shapes),
        in_specs=[vmem] * len(shapes),
        out_specs=(hbm,) * len(shapes),
        scratch_shapes=[dma((len(shapes),))],
        name="hand_on",
    )(*(pltpu.with_memory_space_constraint(x, pltpu.VMEM) for x in outs))


def layer(n, m, *args):
    tokens, query_weight, key_cache = args[0], args[2], args[7]
    expert_gate, side_gate = args[14], args[17]
    seqs, width = tokens.shape
    lanes = (width // n, width // m, query_weight.shape[1], key_cache.shape[2])
    lanes += (key_cache.shape[3], expert_gate.shape[2], side_gate.shape[1])
    lanes += (query_weight.shape[1] // 2,)
    rows = (seqs, key_cache.shape[1])
    held = 2 * sum(a.size for a in args[2:] if a.dtype == BF16) + 2 * key_cache.size
    aligned = all(x % 128 == 0 for x in lanes) and all(x % 8 == 0 for x in rows)
    if n > 1 and m > 1 and aligned and expert_gate.shape[0] == 1 and held < 48 * 1024 * 1024:
        return fused(n, m, *args)
    return body(*args)


def solution(mesh):
    in_specs = (
        P("ep", None),
        P(),
        P("ep", "tp"),
        P("ep", "tp"),
        P("ep", "tp"),
        P(),
        P("tp"),
        P("ep", "tp", None, None),
        P("ep", "tp", None, None),
        P("ep"),
        P("tp", None),
        P(),
        P("ep", None),
        P("ep", None),
        P("ep", None, "tp"),
        P("ep", None, "tp"),
        P("ep", "tp", None),
        P(None, "tp"),
        P(None, "tp"),
        P("tp", None),
        P(),
    )
    out_specs = (P("ep", "tp"), P("ep", "tp"), P("ep", "tp"))
    return jax.shard_map(
        lambda *args: layer(mesh.shape["ep"], mesh.shape["tp"], *args),
        mesh=mesh,
        in_specs=in_specs,
        out_specs=out_specs,
        check_vma=False,
    )
```

```python
import jax
import jax.numpy as jnp
from jax import lax
from jax.experimental import pallas as pl
from jax.experimental.pallas import tpu as pltpu
from jax.sharding import PartitionSpec as P

DH = 128


epsilon = 1e-06


def rms_scale(values, scale_gain):
    mean_square = jnp.mean(values * values, axis=-1, keepdims=True)
    return values * lax.rsqrt(mean_square + epsilon) * scale_gain


def body(
    tokens,
    attn_gain,
    query_weight,
    key_weight,
    value_weight,
    query_gain,
    stick_bias,
    key_cache,
    value_cache,
    lengths,
    out_weight,
    mix_gain,
    route_ids,
    route_weights,
    expert_gate,
    expert_up,
    expert_down,
    side_gate,
    side_up,
    side_down,
    branch_gate,
):
    seq_count, model_width = tokens.shape
    head_cols = query_weight.shape[1]
    heads_local = key_cache.shape[1]
    cache_slots = key_cache.shape[2]
    stream = tokens.astype(jnp.float32)
    normed = rms_scale(stream, attn_gain).astype(jnp.bfloat16)
    stacked = jnp.concatenate([query_weight, key_weight, value_weight], axis=1)
    columns = lax.all_to_all(normed, "ep", split_axis=1, concat_axis=0, tiled=True)
    picked = columns
    projected = lax.psum_scatter(
        jnp.dot(picked, stacked, preferred_element_type=jnp.float32),
        "ep",
        scatter_dimension=0,
        tiled=True,
    )
    query_rows = projected[:, :head_cols].astype(jnp.bfloat16)
    fresh_keys = projected[:, head_cols : 2 * head_cols].astype(jnp.bfloat16)
    new_values = projected[:, 2 * head_cols :].astype(jnp.bfloat16)
    new_keys = rms_scale(fresh_keys.astype(jnp.float32).reshape(seq_count, heads_local, DH), 1.0)
    new_keys = new_keys.astype(jnp.bfloat16).reshape(seq_count, head_cols)
    query_heads = rms_scale(
        query_rows.astype(jnp.float32).reshape(seq_count, heads_local, DH), query_gain
    )
    query_heads = query_heads.astype(jnp.bfloat16)
    scores = jnp.einsum("shd,shld->shl", query_heads, key_cache, preferred_element_type=jnp.float32)
    scores = scores * DH ** (-0.5) + stick_bias[None, :, None]
    positions = jnp.arange(cache_slots, dtype=jnp.int32)
    visible = positions[None, None, :] < lengths[:, None, None]
    log_rest = jnp.where(visible, jax.nn.log_sigmoid(-scores), 0.0)
    log_between = lax.cumsum(log_rest, axis=2, reverse=True) - log_rest
    stick = jnp.where(visible, jnp.exp(jax.nn.log_sigmoid(scores) + log_between), 0.0).astype(
        jnp.bfloat16
    )
    attended = jnp.einsum("shl,shld->shd", stick, value_cache, preferred_element_type=jnp.float32)
    attended = attended.astype(jnp.bfloat16).reshape(seq_count, head_cols)
    attn_proj = lax.psum(
        jnp.dot(attended, out_weight, preferred_element_type=jnp.float32).astype(jnp.bfloat16), "tp"
    ).astype(jnp.float32)
    middle = (stream + attn_proj).astype(jnp.bfloat16)
    normed_mix = rms_scale(middle.astype(jnp.float32), mix_gain).astype(jnp.bfloat16)
    side_gate_pre = jnp.dot(normed_mix, side_gate, preferred_element_type=jnp.float32)
    side_up_pre = jnp.dot(normed_mix, side_up, preferred_element_type=jnp.float32)
    side_hidden = (jax.nn.silu(side_gate_pre) * side_up_pre).astype(jnp.bfloat16)
    side_term = jnp.dot(side_hidden, side_down, preferred_element_type=jnp.float32)
    switch = jax.nn.sigmoid(
        jnp.sum(normed_mix.astype(jnp.float32) * branch_gate, axis=1, keepdims=True)
    )
    experts = lax.axis_size("ep")
    top_count = route_ids.shape[1]
    capacity = max(2, 2 * top_count * seq_count // experts)
    flat_ids = route_ids.reshape(-1)
    onehot = (flat_ids[:, None] == jnp.arange(experts, dtype=jnp.int32)[None, :]).astype(jnp.int32)
    before = jnp.cumsum(onehot, axis=0) - onehot
    slot_index = jnp.sum(before * onehot, axis=1)
    target = flat_ids * capacity + slot_index
    route_map = (
        target[:, None] == jnp.arange(experts * capacity, dtype=jnp.int32)[None, :]
    ).astype(jnp.bfloat16)
    dispatch = jnp.sum(route_map.reshape(seq_count, top_count, experts * capacity), axis=1).T
    outbox = jnp.dot(dispatch, normed_mix, preferred_element_type=jnp.float32).astype(jnp.bfloat16)
    outbox = outbox.reshape(experts, capacity, model_width)
    col_width = model_width // lax.axis_size("tp")
    col_offset = lax.axis_index("tp") * col_width
    arrived = lax.all_to_all(outbox, "ep", split_axis=0, concat_axis=0, tiled=True)
    slot_rows = arrived.reshape(experts * capacity, model_width)
    gate_pre = jnp.dot(slot_rows, expert_gate[0], preferred_element_type=jnp.float32)
    up_pre = jnp.dot(slot_rows, expert_up[0], preferred_element_type=jnp.float32)
    hidden = (jax.nn.silu(gate_pre) * up_pre).astype(jnp.bfloat16)
    expert_term = jnp.dot(hidden, expert_down[0], preferred_element_type=jnp.float32)
    expert_part, side_part = (
        lax.psum_scatter(
            expert_term.astype(jnp.bfloat16), "tp", scatter_dimension=1, tiled=True
        ).astype(jnp.float32),
        lax.psum_scatter(
            side_term.astype(jnp.bfloat16), "tp", scatter_dimension=1, tiled=True
        ).astype(jnp.float32),
    )
    returned = lax.all_to_all(
        expert_part.astype(jnp.bfloat16).reshape(experts, capacity, col_width),
        "ep",
        split_axis=0,
        concat_axis=0,
        tiled=True,
    )
    picked = jnp.dot(
        route_map,
        returned.reshape(experts * capacity, col_width),
        preferred_element_type=jnp.float32,
    )
    routed = jnp.sum(
        route_weights[:, :, None] * picked.reshape(seq_count, top_count, col_width), axis=1
    )
    middle_cols = lax.dynamic_slice_in_dim(middle, col_offset, col_width, 1).astype(jnp.float32)
    mixed = (middle_cols + routed + switch * side_part).astype(jnp.bfloat16)
    return (mixed, new_keys, new_values)


MESH = pl.DeviceIdType.MESH
F32 = jnp.float32
BF16 = jnp.bfloat16


def softplus(values):
    return jnp.maximum(values, 0.0) + jnp.log1p(jnp.exp(-jnp.abs(values)))


def silu(values):
    return values / (1.0 + jnp.exp(-values))


def as_columns(rows):
    count = rows.shape[1]
    own = lax.broadcasted_iota(jnp.int32, (count, count), 0) == lax.broadcasted_iota(
        jnp.int32, (count, count), 1
    )
    rows = rows.astype(F32)
    return [
        jnp.sum(jnp.where(own, rows[i : i + 1], 0.0), axis=1, keepdims=True)
        for i in range(rows.shape[0])
    ]


class Phases:
    def __init__(self):
        self.scope = None

    def __call__(self, name):
        if self.scope is not None:
            self.scope.__exit__(None, None, None)
        self.scope = jax.named_scope(name) if name else None
        if self.scope is not None:
            self.scope.__enter__()


def stack_rows(buffer):
    return jnp.concatenate([buffer[i].astype(F32) for i in range(buffer.shape[0])], axis=0)


def layer_kernel(
    n,
    m,
    tokens_hbm,
    attn_gain_hbm,
    query_gain_hbm,
    bias_hbm,
    lengths_hbm,
    mix_gain_hbm,
    ids_hbm,
    weights_hbm,
    branch_hbm,
    wq_hbm,
    wk_hbm,
    wv_hbm,
    key_hbm,
    value_hbm,
    out_hbm,
    gate_hbm,
    up_hbm,
    down_hbm,
    side_gate_hbm,
    side_up_hbm,
    side_down_hbm,
    mixed_ref,
    new_keys_ref,
    new_values_ref,
    tokens_ref,
    rows_ref,
    query_gain_ref,
    bias_ref,
    lengths_ref,
    ids_ref,
    weights_ref,
    proj_w,
    keys,
    turned,
    values,
    out_w,
    expert_w,
    down_w,
    side_w,
    side_down_w,
    col_send,
    col_recv,
    query_send,
    query_recv,
    proj_send,
    proj_recv,
    reduce_buf,
    mid_cols,
    mix_send,
    mix_recv,
    slot_rows,
    pre,
    slot_cols,
    side_cols,
    side_send,
    side_recv,
    back_send,
    back_recv,
    load_sem,
    send_sem,
    recv_sem,
):
    ep = lax.axis_index("ep")
    tp = lax.axis_index("tp")
    seqs, width = tokens_ref.shape
    heads, dh, slots = turned.shape[0], turned.shape[2], turned.shape[3]
    cols = width // n
    out_cols = width // m
    parts = reduce_buf.shape[0]
    part_cols = width // parts

    phase_name = Phases()
    phase_name("greet")
    def load(k, whole, *pairs, priority=1):
        for src, dst in pairs:
            pltpu.make_async_copy(src, dst, load_sem.at[k]).start(priority=priority)
        return pltpu.make_async_copy(whole, whole, load_sem.at[k])

    tokens_load = load(0, tokens_ref, (tokens_hbm, tokens_ref), priority=0)
    gains = (attn_gain_hbm, mix_gain_hbm, branch_hbm)
    rows_load = load(1, rows_ref, *((x, rows_ref.at[i]) for i, x in enumerate(gains)), priority=0)
    barrier = pltpu.get_barrier_semaphore()
    for d in range(1, n):
        pl.semaphore_signal(barrier, inc=1, device_id=(lax.rem(ep + d, n), tp), device_id_type=MESH)
    for d in range(1, m):
        pl.semaphore_signal(barrier, inc=1, device_id=(ep, lax.rem(tp + d, m)), device_id_type=MESH)
    small = (
        (ids_hbm, ids_ref),
        (weights_hbm, weights_ref),
        (query_gain_hbm, query_gain_ref),
        (bias_hbm, bias_ref),
        (lengths_hbm, lengths_ref),
    )
    small_loads = [load(2 + i, x[1], x, priority=0) for i, x in enumerate(small)]
    proj_load = load(
        7,
        proj_w,
        *((w, proj_w.at[i]) for i, w in enumerate((wq_hbm, wk_hbm, wv_hbm))),
        priority=0,
    )
    key_load = load(8, keys, *((key_hbm.at[i], keys.at[i]) for i in range(seqs)))
    value_load = load(9, values, *((value_hbm.at[i], values.at[:, i]) for i in range(seqs)))

    def remote(sem, src, dst, target, arrival=None):
        copy = pltpu.make_async_remote_copy(
            src_ref=src,
            dst_ref=dst,
            send_sem=send_sem.at[sem],
            recv_sem=recv_sem.at[sem if arrival is None else arrival],
            device_id=target,
            device_id_type=MESH,
        )
        copy.start()

    def sent(sem, whole):
        pltpu.make_async_copy(whole, whole, send_sem.at[sem]).wait()

    def arrived(sem, whole):
        pltpu.make_async_copy(whole, whole, recv_sem.at[sem]).wait()

    upper = ep // (n // 2)
    far_first = []
    for k in range(n - 1):
        low = n - 2 - k + (n - 1 - k - ep + n - 1) // n
        high = k + (k - ep + n) // n
        far_first.append((1 - upper) * low + upper * high)

    def ep_scatter(sem, send, recv, arrival=None):
        for j in far_first:
            remote(sem, send.at[j], recv.at[ep], (j, tp), arrival)

    others = pl.ds(0, n - 1)
    fellows = pl.ds(0, m - 1)
    groups = query_send.shape[0]
    s_first, s_plane, s_rows, s_proj = range(4)
    r_col, r_proj, r_side, r_back, r_near, r_query = range(6)
    r_reduce = r_query + groups
    r_mix = r_reduce + parts

    tokens_load.wait()
    rows_load.wait()
    attn_gain, mix_gain, branch_gate = (rows_ref[i] for i in range(3))
    stream = tokens_ref[...].astype(F32)
    normed = rms_scale(stream, attn_gain)
    for j in range(n):
        col_send[j] = normed[:, j * cols : (j + 1) * cols].astype(BF16)
    col_recv[ep] = col_send[ep]
    phase_name("barrier")
    pl.semaphore_wait(barrier, (n - 1) + (m - 1))
    phase_name("col_send")
    ep_scatter(s_first, col_send, col_recv, r_col)

    for copy in small_loads:
        copy.wait()
    later = lax.broadcasted_iota(jnp.int32, (slots, slots), 0) > lax.broadcasted_iota(
        jnp.int32, (slots, slots), 1
    )
    later = jnp.where(later, 1.0, 0.0).astype(BF16)
    capacity = mix_send.shape[2]
    lane_expert = lax.broadcasted_iota(jnp.int32, (seqs, n), 1).astype(F32)
    lane_slot = lax.broadcasted_iota(jnp.int32, (seqs, n * capacity), 1).astype(F32)
    row_slot = lax.broadcasted_iota(jnp.int32, (n * capacity, seqs), 0).astype(F32)
    first = lax.broadcasted_iota(jnp.int32, (seqs, seqs), 0)
    second = lax.broadcasted_iota(jnp.int32, (seqs, seqs), 1)
    weights = as_columns(weights_ref[...])
    ids = as_columns(ids_ref[...])
    named = [jnp.where(lane_expert == i, 1.0, 0.0) for i in ids]
    before = jnp.dot(
        jnp.where(second < first, 1.0, 0.0).astype(BF16),
        sum(named).astype(BF16),
        preferred_element_type=F32,
    )
    targets = [
        i * float(capacity) + jnp.sum(before * x, axis=1, keepdims=True) for i, x in zip(ids, named)
    ]
    route_map = jnp.concatenate(
        [jnp.where(lane_slot == t, 1.0, 0.0) for t in targets], axis=0
    ).astype(BF16)
    dispatch = sum(
        jnp.where(
            row_slot == jnp.sum(jnp.where(first == second, t, 0.0), axis=0, keepdims=True), 1.0, 0.0
        )
        for t in targets
    ).astype(BF16)
    proj_load.wait()
    phase_name("col_wait")
    arrived(r_col, col_recv.at[others])
    phase_name("project")
    picked = stack_rows(col_recv).astype(BF16)

    half = query_send.shape[3]
    part = jnp.dot(picked, proj_w[0], preferred_element_type=F32).astype(BF16)
    sent(s_first, col_send.at[others])
    for g in range(groups):
        for j in range(n):
            query_send[g, j] = part[j * seqs : (j + 1) * seqs, g * half : (g + 1) * half]
        query_recv[g, ep] = query_send[g, ep]
        ep_scatter(s_first, query_send.at[g], query_recv.at[g], r_query + g)
    phase_name("turn")
    out_load = load(0, out_w, (out_hbm, out_w))
    side_load = load(1, side_w, (side_gate_hbm, side_w.at[0]), (side_up_hbm, side_w.at[1]))
    side_down_load = load(2, side_down_w, (side_down_hbm, side_down_w))
    expert_load = load(3, expert_w, (gate_hbm.at[0], expert_w.at[0]), (up_hbm.at[0], expert_w.at[1]))
    down_load = load(4, down_w, (down_hbm.at[0], down_w))
    for i in (1, 2):
        part = jnp.dot(picked, proj_w[i], preferred_element_type=F32)
        for j in range(n):
            proj_send[i - 1, j] = part[j * seqs : (j + 1) * seqs].astype(BF16)
        proj_recv[i - 1, ep] = proj_send[i - 1, ep]
    key_load.wait()
    for s in range(seqs):
        for h in range(heads):
            turned[h, s] = keys[s, h].T
    value_load.wait()

    def collect(recv):
        total = recv[0].astype(F32)
        for j in range(1, n):
            total = total + recv[j].astype(F32)
        return total.astype(BF16).astype(F32)

    query_row = lax.broadcasted_iota(jnp.int32, (seqs, dh), 0)
    slot_row = lax.broadcasted_iota(jnp.int32, (seqs, slots), 0)
    position = lax.broadcasted_iota(jnp.int32, (seqs, slots), 1)
    lengths = as_columns(lengths_ref[...])[0].astype(jnp.int32)
    visible = position < lengths
    scale = dh ** (-0.5)
    some = half // dh
    score_rows, rest_rows = [], []
    for g in range(groups):
        phase_name("query_wait")
        arrived(r_query + g, query_recv.at[g, others])
        phase_name("scores")
        query = collect(query_recv.at[g])
        if g == 0:
            for i in range(2):
                ep_scatter(s_proj, proj_send.at[i], proj_recv.at[i], r_proj)
        for k in range(some):
            h = g * some + k
            q = rms_scale(query[:, k * dh : (k + 1) * dh], query_gain_ref[...])
            spread = jnp.concatenate(
                [jnp.where(query_row == s, q, 0.0).astype(BF16) for s in range(seqs)], axis=1
            )
            score = jnp.dot(
                spread, turned[h].reshape(seqs * dh, slots), preferred_element_type=F32
            )
            score = score * scale + bias_ref[0:1, h : h + 1]
            full = -softplus(score)
            score_rows.append(score + full)
            rest_rows.append(jnp.where(visible, full, 0.0))
    rest = jnp.concatenate(rest_rows, axis=0)
    high = rest.astype(BF16)
    left = rest - high.astype(F32)
    middle_part = left.astype(BF16)
    low = (left - middle_part.astype(F32)).astype(BF16)
    pieces = jnp.dot(
        jnp.concatenate([high, middle_part, low], axis=0), later, preferred_element_type=F32
    )
    count = seqs * heads
    between = pieces[:count] + pieces[count : 2 * count] + pieces[2 * count :]
    attended = []
    for h in range(heads):
        stick = jnp.where(
            visible, jnp.exp(score_rows[h] + between[h * seqs : (h + 1) * seqs]), 0.0
        )
        spread = jnp.concatenate(
            [jnp.where(slot_row == s, stick, 0.0).astype(BF16) for s in range(seqs)], axis=1
        )
        attended.append(
            jnp.dot(spread, values[h].reshape(seqs * slots, dh), preferred_element_type=F32)
        )
    attended = jnp.concatenate(attended, axis=1).astype(BF16)
    phase_name("out_proj")
    out_load.wait()
    for t in range(parts):
        reduce_buf[t, tp] = jnp.dot(
            attended, out_w[:, t * part_cols : (t + 1) * part_cols], preferred_element_type=F32
        ).astype(BF16)
        for d in range(1, m):
            own = reduce_buf.at[t, tp]
            remote(s_plane, own, own, (ep, lax.rem(tp + d, m)), r_reduce + t)

    middle = []
    for t in range(parts):
        phase_name("reduce_wait")
        arrived(r_reduce + t, reduce_buf.at[t, fellows])
        phase_name("mix")
        total = sum(reduce_buf[t, i].astype(F32) for i in range(m))
        part = (stream[:, t * part_cols : (t + 1) * part_cols] + total).astype(BF16)
        outbox = jnp.dot(dispatch, part, preferred_element_type=F32)
        for j in range(n):
            mix_send[t, j] = outbox[j * capacity : (j + 1) * capacity].astype(BF16)
        mix_recv[t, ep] = mix_send[t, ep]
        ep_scatter(s_rows, mix_send.at[t], mix_recv.at[t], r_mix + t)
        middle.append(part.astype(F32))
    middle = jnp.concatenate(middle, axis=1)
    for t in range(m):
        mid_cols[t] = middle[:, t * out_cols : (t + 1) * out_cols]

    phase_name("side")
    normed_mix = rms_scale(middle, mix_gain).astype(BF16)
    side_load.wait()
    side_down_load.wait()
    side_hidden = silu(
        jnp.dot(normed_mix, side_w[0], preferred_element_type=F32)
    ) * jnp.dot(normed_mix, side_w[1], preferred_element_type=F32)
    side_term = jnp.dot(side_hidden.astype(BF16), side_down_w[...], preferred_element_type=F32)
    switch = jnp.sum(normed_mix.astype(F32) * branch_gate, axis=1, keepdims=True)
    switch = 1.0 / (1.0 + jnp.exp(-switch))
    for t in range(m):
        side_cols[t] = switch * side_term[:, t * out_cols : (t + 1) * out_cols]
    sent(s_plane, reduce_buf.at[:, fellows])
    for d in range(1, m):
        t = lax.rem(tp + d, m)
        side_send[d - 1] = side_cols[t].astype(BF16)
        remote(s_plane, side_send.at[d - 1], side_recv.at[d - 1], (ep, t), r_side)

    phase_name("settle")
    expert_load.wait()
    down_load.wait()
    sent(s_first, query_send.at[:, others])

    squares = None
    for t in range(parts):
        phase_name("rows_wait")
        arrived(r_mix + t, mix_recv.at[t, others])
        phase_name("expert")
        for j in range(n):
            slot_rows[t, j * capacity : (j + 1) * capacity, :] = mix_recv[t, j].astype(F32)
        span = slice(t * part_cols, (t + 1) * part_cols)
        rows = slot_rows[t]
        square = jnp.sum(rows * rows, axis=1, keepdims=True)
        rows = (rows * mix_gain[:, span]).astype(BF16)
        for i in range(2):
            share = jnp.dot(rows, expert_w[i, span, :], preferred_element_type=F32)
            pre[i] = share if t == 0 else pre[i] + share
        squares = square if t == 0 else squares + square
        if t == 0:
            sent(s_plane, side_send.at[...])
    sent(s_rows, mix_send.at[:, others])
    gate_pre, up_pre = pre[0], pre[1]
    factor = lax.rsqrt(squares / width + epsilon)
    hidden = (silu(gate_pre * factor) * (up_pre * factor)).astype(BF16)
    for t in range(m):
        expert_term = jnp.dot(
            hidden, down_w[:, t * out_cols : (t + 1) * out_cols], preferred_element_type=F32
        )
        for j in range(n):
            back_send[t, j] = expert_term[j * capacity : (j + 1) * capacity].astype(BF16)
        for k in range(n - 1):
            j = k + (k - ep + n) // n
            remote(s_rows, back_send.at[t, j], back_recv.at[tp, ep], (j, t), r_back)
    for d in range(1, m):
        t = lax.rem(tp + d, m)
        remote(s_plane, back_send.at[t, ep], back_recv.at[tp, ep], (ep, t), r_near)
    back_recv[tp, ep] = back_send[tp, ep]
    phase_name("side_wait")
    result = mid_cols[tp] + side_cols[tp]
    arrived(r_side, side_recv.at[...])
    for d in range(1, m):
        result = result + side_recv[d - 1].astype(F32)
    phase_name("new_keys")
    arrived(r_proj, proj_recv.at[:, others])
    key_rows = collect(proj_recv.at[0])
    for h in range(heads):
        part = slice(h * dh, (h + 1) * dh)
        new_keys_ref[:, part] = rms_scale(key_rows[:, part], 1.0).astype(BF16)
    new_values_ref[...] = collect(proj_recv.at[1]).astype(BF16)
    sent(s_proj, proj_send.at[:, others])
    phase_name("back_wait")
    arrived(r_near, back_recv.at[fellows, 0])
    arrived(r_back, back_recv.at[:, others])
    phase_name("combine")
    for j in range(n):
        slot_cols[j * capacity : (j + 1) * capacity, :] = sum(
            back_recv[i, j].astype(F32) for i in range(m)
        )
    chosen = jnp.dot(route_map, slot_cols[...].astype(BF16), preferred_element_type=F32)
    for k, w in enumerate(weights):
        result = result + w * chosen[k * seqs : (k + 1) * seqs]
    mixed_ref[...] = result.astype(BF16)
    phase_name("drain")
    sent(s_plane, back_send.at[fellows, 0])
    sent(s_rows, back_send.at[:, others])
    phase_name(None)


def hand_on(count, *refs):
    sources, targets, sem = refs[:count], refs[count : 2 * count], refs[-1]
    copies = [
        pltpu.make_async_copy(src, dst, sem.at[i])
        for i, (src, dst) in enumerate(zip(sources, targets))
    ]
    for copy in copies:
        copy.start()
    for copy in copies:
        copy.wait()


def fused(n, m, *args):
    (
        tokens,
        attn_gain,
        query_weight,
        key_weight,
        value_weight,
        query_gain,
        stick_bias,
        key_cache,
        value_cache,
        lengths,
        out_weight,
        mix_gain,
        route_ids,
        route_weights,
        expert_gate,
        expert_up,
        expert_down,
        side_gate,
        side_up,
        side_down,
        branch_gate,
    ) = args
    seqs, width = tokens.shape
    _, heads, slots, dh = key_cache.shape
    head_cols = query_weight.shape[1]
    out_cols = width // m
    capacity = max(2, 2 * route_ids.shape[1] * seqs // n)
    parts = 2
    groups = 2
    vmem = pl.BlockSpec(memory_space=pltpu.VMEM)
    hbm = pl.BlockSpec(memory_space=pl.ANY)
    dma = pltpu.SemaphoreType.DMA

    def scratch(*shape, dtype=BF16):
        return pltpu.VMEM(shape, dtype)

    small = (
        tokens,
        attn_gain.reshape(1, width),
        query_gain.reshape(1, dh),
        stick_bias.reshape(1, heads),
        lengths.reshape(1, seqs),
        mix_gain.reshape(1, width),
        route_ids.T,
        route_weights.T,
        branch_gate.reshape(1, width),
    )
    shapes = ((seqs, out_cols), (seqs, head_cols), (seqs, head_cols))
    outs = pl.pallas_call(
        lambda *refs: layer_kernel(n, m, *refs),
        out_shape=tuple(pltpu.VMEM(shape, BF16) for shape in shapes),
        in_specs=[hbm] * 21,
        out_specs=(vmem, vmem, vmem),
        scratch_shapes=[
            scratch(seqs, width),
            scratch(3, 1, width, dtype=F32),
            *(scratch(*x.shape, dtype=x.dtype) for x in (*small[2:5], *small[6:8])),
            scratch(3, *query_weight.shape),
            scratch(*key_cache.shape),
            scratch(heads, seqs, dh, slots),
            scratch(heads, seqs, slots, dh),
            scratch(*out_weight.shape),
            scratch(2, *expert_gate.shape[1:]),
            scratch(*expert_down.shape[1:]),
            scratch(2, *side_gate.shape),
            scratch(*side_down.shape),
            scratch(n, seqs, width // n),
            scratch(n, seqs, width // n),
            scratch(groups, n, seqs, head_cols // groups),
            scratch(groups, n, seqs, head_cols // groups),
            scratch(2, n, seqs, head_cols),
            scratch(2, n, seqs, head_cols),
            scratch(parts, m, seqs, width // parts),
            scratch(m, seqs, out_cols, dtype=F32),
            scratch(parts, n, capacity, width // parts),
            scratch(parts, n, capacity, width // parts),
            scratch(parts, n * capacity, width // parts, dtype=F32),
            scratch(2, n * capacity, expert_gate.shape[2], dtype=F32),
            scratch(n * capacity, out_cols, dtype=F32),
            scratch(m, seqs, out_cols, dtype=F32),
            scratch(m - 1, seqs, out_cols),
            scratch(m - 1, seqs, out_cols),
            scratch(m, n, capacity, out_cols),
            scratch(m, n, capacity, out_cols),
            dma((10,)),
            dma((4,)),
            dma((5 + groups + 2 * parts,)),
        ],
        compiler_params=pltpu.CompilerParams(
            collective_id=0, has_side_effects=True, vmem_limit_bytes=60 * 1024 * 1024
        ),
        name="layer",
    )(
        *small,
        query_weight,
        key_weight,
        value_weight,
        key_cache,
        value_cache,
        out_weight,
        expert_gate,
        expert_up,
        expert_down,
        side_gate,
        side_up,
        side_down,
    )
    return pl.pallas_call(
        lambda *refs: hand_on(len(shapes), *refs),
        out_shape=tuple(jax.ShapeDtypeStruct(shape, BF16) for shape in shapes),
        in_specs=[vmem] * len(shapes),
        out_specs=(hbm,) * len(shapes),
        scratch_shapes=[dma((len(shapes),))],
        name="hand_on",
    )(*(pltpu.with_memory_space_constraint(x, pltpu.VMEM) for x in outs))


def layer(n, m, *args):
    tokens, query_weight, key_cache = args[0], args[2], args[7]
    expert_gate, side_gate = args[14], args[17]
    seqs, width = tokens.shape
    lanes = (width // n, width // m, query_weight.shape[1], key_cache.shape[2])
    lanes += (key_cache.shape[3], expert_gate.shape[2], side_gate.shape[1])
    lanes += (query_weight.shape[1] // 2, width // 2)
    rows = (seqs, key_cache.shape[1])
    held = 2 * sum(a.size for a in args[2:] if a.dtype == BF16) + 2 * key_cache.size
    aligned = all(x % 128 == 0 for x in lanes) and all(x % 8 == 0 for x in rows)
    if n > 1 and m > 1 and aligned and expert_gate.shape[0] == 1 and held < 48 * 1024 * 1024:
        return fused(n, m, *args)
    return body(*args)


def solution(mesh):
    in_specs = (
        P("ep", None),
        P(),
        P("ep", "tp"),
        P("ep", "tp"),
        P("ep", "tp"),
        P(),
        P("tp"),
        P("ep", "tp", None, None),
        P("ep", "tp", None, None),
        P("ep"),
        P("tp", None),
        P(),
        P("ep", None),
        P("ep", None),
        P("ep", None, "tp"),
        P("ep", None, "tp"),
        P("ep", "tp", None),
        P(None, "tp"),
        P(None, "tp"),
        P("tp", None),
        P(),
    )
    out_specs = (P("ep", "tp"), P("ep", "tp"), P("ep", "tp"))
    return jax.shard_map(
        lambda *args: layer(mesh.shape["ep"], mesh.shape["tp"], *args),
        mesh=mesh,
        in_specs=in_specs,
        out_specs=out_specs,
        check_vma=False,
    )
```

```python
import jax
import jax.numpy as jnp
from jax import lax
from jax.experimental import pallas as pl
from jax.experimental.pallas import tpu as pltpu
from jax.sharding import PartitionSpec as P

DH = 128


epsilon = 1e-06


def rms_scale(values, scale_gain):
    mean_square = jnp.mean(values * values, axis=-1, keepdims=True)
    return values * lax.rsqrt(mean_square + epsilon) * scale_gain


def body(
    tokens,
    attn_gain,
    query_weight,
    key_weight,
    value_weight,
    query_gain,
    stick_bias,
    key_cache,
    value_cache,
    lengths,
    out_weight,
    mix_gain,
    route_ids,
    route_weights,
    expert_gate,
    expert_up,
    expert_down,
    side_gate,
    side_up,
    side_down,
    branch_gate,
):
    seq_count, model_width = tokens.shape
    head_cols = query_weight.shape[1]
    heads_local = key_cache.shape[1]
    cache_slots = key_cache.shape[2]
    stream = tokens.astype(jnp.float32)
    normed = rms_scale(stream, attn_gain).astype(jnp.bfloat16)
    stacked = jnp.concatenate([query_weight, key_weight, value_weight], axis=1)
    columns = lax.all_to_all(normed, "ep", split_axis=1, concat_axis=0, tiled=True)
    picked = columns
    projected = lax.psum_scatter(
        jnp.dot(picked, stacked, preferred_element_type=jnp.float32),
        "ep",
        scatter_dimension=0,
        tiled=True,
    )
    query_rows = projected[:, :head_cols].astype(jnp.bfloat16)
    fresh_keys = projected[:, head_cols : 2 * head_cols].astype(jnp.bfloat16)
    new_values = projected[:, 2 * head_cols :].astype(jnp.bfloat16)
    new_keys = rms_scale(fresh_keys.astype(jnp.float32).reshape(seq_count, heads_local, DH), 1.0)
    new_keys = new_keys.astype(jnp.bfloat16).reshape(seq_count, head_cols)
    query_heads = rms_scale(
        query_rows.astype(jnp.float32).reshape(seq_count, heads_local, DH), query_gain
    )
    query_heads = query_heads.astype(jnp.bfloat16)
    scores = jnp.einsum("shd,shld->shl", query_heads, key_cache, preferred_element_type=jnp.float32)
    scores = scores * DH ** (-0.5) + stick_bias[None, :, None]
    positions = jnp.arange(cache_slots, dtype=jnp.int32)
    visible = positions[None, None, :] < lengths[:, None, None]
    log_rest = jnp.where(visible, jax.nn.log_sigmoid(-scores), 0.0)
    log_between = lax.cumsum(log_rest, axis=2, reverse=True) - log_rest
    stick = jnp.where(visible, jnp.exp(jax.nn.log_sigmoid(scores) + log_between), 0.0).astype(
        jnp.bfloat16
    )
    attended = jnp.einsum("shl,shld->shd", stick, value_cache, preferred_element_type=jnp.float32)
    attended = attended.astype(jnp.bfloat16).reshape(seq_count, head_cols)
    attn_proj = lax.psum(
        jnp.dot(attended, out_weight, preferred_element_type=jnp.float32).astype(jnp.bfloat16), "tp"
    ).astype(jnp.float32)
    middle = (stream + attn_proj).astype(jnp.bfloat16)
    normed_mix = rms_scale(middle.astype(jnp.float32), mix_gain).astype(jnp.bfloat16)
    side_gate_pre = jnp.dot(normed_mix, side_gate, preferred_element_type=jnp.float32)
    side_up_pre = jnp.dot(normed_mix, side_up, preferred_element_type=jnp.float32)
    side_hidden = (jax.nn.silu(side_gate_pre) * side_up_pre).astype(jnp.bfloat16)
    side_term = jnp.dot(side_hidden, side_down, preferred_element_type=jnp.float32)
    switch = jax.nn.sigmoid(
        jnp.sum(normed_mix.astype(jnp.float32) * branch_gate, axis=1, keepdims=True)
    )
    experts = lax.axis_size("ep")
    top_count = route_ids.shape[1]
    capacity = max(2, 2 * top_count * seq_count // experts)
    flat_ids = route_ids.reshape(-1)
    onehot = (flat_ids[:, None] == jnp.arange(experts, dtype=jnp.int32)[None, :]).astype(jnp.int32)
    before = jnp.cumsum(onehot, axis=0) - onehot
    slot_index = jnp.sum(before * onehot, axis=1)
    target = flat_ids * capacity + slot_index
    route_map = (
        target[:, None] == jnp.arange(experts * capacity, dtype=jnp.int32)[None, :]
    ).astype(jnp.bfloat16)
    dispatch = jnp.sum(route_map.reshape(seq_count, top_count, experts * capacity), axis=1).T
    outbox = jnp.dot(dispatch, normed_mix, preferred_element_type=jnp.float32).astype(jnp.bfloat16)
    outbox = outbox.reshape(experts, capacity, model_width)
    col_width = model_width // lax.axis_size("tp")
    col_offset = lax.axis_index("tp") * col_width
    arrived = lax.all_to_all(outbox, "ep", split_axis=0, concat_axis=0, tiled=True)
    slot_rows = arrived.reshape(experts * capacity, model_width)
    gate_pre = jnp.dot(slot_rows, expert_gate[0], preferred_element_type=jnp.float32)
    up_pre = jnp.dot(slot_rows, expert_up[0], preferred_element_type=jnp.float32)
    hidden = (jax.nn.silu(gate_pre) * up_pre).astype(jnp.bfloat16)
    expert_term = jnp.dot(hidden, expert_down[0], preferred_element_type=jnp.float32)
    expert_part, side_part = (
        lax.psum_scatter(
            expert_term.astype(jnp.bfloat16), "tp", scatter_dimension=1, tiled=True
        ).astype(jnp.float32),
        lax.psum_scatter(
            side_term.astype(jnp.bfloat16), "tp", scatter_dimension=1, tiled=True
        ).astype(jnp.float32),
    )
    returned = lax.all_to_all(
        expert_part.astype(jnp.bfloat16).reshape(experts, capacity, col_width),
        "ep",
        split_axis=0,
        concat_axis=0,
        tiled=True,
    )
    picked = jnp.dot(
        route_map,
        returned.reshape(experts * capacity, col_width),
        preferred_element_type=jnp.float32,
    )
    routed = jnp.sum(
        route_weights[:, :, None] * picked.reshape(seq_count, top_count, col_width), axis=1
    )
    middle_cols = lax.dynamic_slice_in_dim(middle, col_offset, col_width, 1).astype(jnp.float32)
    mixed = (middle_cols + routed + switch * side_part).astype(jnp.bfloat16)
    return (mixed, new_keys, new_values)


MESH = pl.DeviceIdType.MESH
F32 = jnp.float32
BF16 = jnp.bfloat16


def softplus(values):
    return jnp.maximum(values, 0.0) + jnp.log1p(jnp.exp(-jnp.abs(values)))


def silu(values):
    return values / (1.0 + jnp.exp(-values))


def as_columns(rows):
    count = rows.shape[1]
    own = lax.broadcasted_iota(jnp.int32, (count, count), 0) == lax.broadcasted_iota(
        jnp.int32, (count, count), 1
    )
    rows = rows.astype(F32)
    return [
        jnp.sum(jnp.where(own, rows[i : i + 1], 0.0), axis=1, keepdims=True)
        for i in range(rows.shape[0])
    ]


class Phases:
    def __init__(self):
        self.scope = None

    def __call__(self, name):
        if self.scope is not None:
            self.scope.__exit__(None, None, None)
        self.scope = jax.named_scope(name) if name else None
        if self.scope is not None:
            self.scope.__enter__()


def stack_rows(buffer):
    return jnp.concatenate([buffer[i].astype(F32) for i in range(buffer.shape[0])], axis=0)


def vector_products(rows, blocks):
    columns = rows.astype(BF16).astype(F32).T
    return jnp.concatenate(
        [
            jnp.sum(blocks[s].astype(F32) * columns[:, s : s + 1], axis=0, keepdims=True)
            for s in range(rows.shape[0])
        ],
        axis=0,
    )


def layer_kernel(
    n,
    m,
    tokens_hbm,
    attn_gain_hbm,
    query_gain_hbm,
    bias_hbm,
    lengths_hbm,
    mix_gain_hbm,
    ids_hbm,
    weights_hbm,
    branch_hbm,
    wq_hbm,
    wk_hbm,
    wv_hbm,
    key_hbm,
    value_hbm,
    out_hbm,
    gate_hbm,
    up_hbm,
    down_hbm,
    side_gate_hbm,
    side_up_hbm,
    side_down_hbm,
    mixed_ref,
    new_keys_ref,
    new_values_ref,
    tokens_ref,
    rows_ref,
    query_gain_ref,
    bias_ref,
    lengths_ref,
    ids_ref,
    weights_ref,
    proj_w,
    keys,
    turned,
    values,
    out_w,
    expert_w,
    down_w,
    side_w,
    side_down_w,
    col_send,
    col_recv,
    query_send,
    query_recv,
    proj_send,
    proj_recv,
    reduce_buf,
    mid_cols,
    mix_send,
    mix_recv,
    slot_rows,
    pre,
    slot_cols,
    side_cols,
    side_send,
    side_recv,
    back_send,
    back_recv,
    load_sem,
    send_sem,
    recv_sem,
):
    ep = lax.axis_index("ep")
    tp = lax.axis_index("tp")
    seqs, width = tokens_ref.shape
    heads, dh, slots = turned.shape[0], turned.shape[2], turned.shape[3]
    cols = width // n
    out_cols = width // m
    parts = reduce_buf.shape[0]
    part_cols = width // parts

    phase_name = Phases()
    phase_name("greet")
    def load(k, whole, *pairs, priority=1):
        for src, dst in pairs:
            pltpu.make_async_copy(src, dst, load_sem.at[k]).start(priority=priority)
        return pltpu.make_async_copy(whole, whole, load_sem.at[k])

    tokens_load = load(0, tokens_ref, (tokens_hbm, tokens_ref), priority=0)
    gains = (attn_gain_hbm, mix_gain_hbm, branch_hbm)
    rows_load = load(1, rows_ref, *((x, rows_ref.at[i]) for i, x in enumerate(gains)), priority=0)
    barrier = pltpu.get_barrier_semaphore()
    for d in range(1, n):
        pl.semaphore_signal(barrier, inc=1, device_id=(lax.rem(ep + d, n), tp), device_id_type=MESH)
    for d in range(1, m):
        pl.semaphore_signal(barrier, inc=1, device_id=(ep, lax.rem(tp + d, m)), device_id_type=MESH)
    small = (
        (ids_hbm, ids_ref),
        (weights_hbm, weights_ref),
        (query_gain_hbm, query_gain_ref),
        (bias_hbm, bias_ref),
        (lengths_hbm, lengths_ref),
    )
    small_loads = [load(2 + i, x[1], x, priority=0) for i, x in enumerate(small)]
    proj_load = load(
        7,
        proj_w,
        *((w, proj_w.at[i]) for i, w in enumerate((wq_hbm, wk_hbm, wv_hbm))),
        priority=0,
    )
    key_load = load(8, keys, *((key_hbm.at[i], keys.at[i]) for i in range(seqs)))
    value_load = load(9, values, *((value_hbm.at[i], values.at[:, i]) for i in range(seqs)))

    def remote(sem, src, dst, target, arrival=None):
        copy = pltpu.make_async_remote_copy(
            src_ref=src,
            dst_ref=dst,
            send_sem=send_sem.at[sem],
            recv_sem=recv_sem.at[sem if arrival is None else arrival],
            device_id=target,
            device_id_type=MESH,
        )
        copy.start()

    def sent(sem, whole):
        pltpu.make_async_copy(whole, whole, send_sem.at[sem]).wait()

    def arrived(sem, whole):
        pltpu.make_async_copy(whole, whole, recv_sem.at[sem]).wait()

    upper = ep // (n // 2)
    far_first = []
    for k in range(n - 1):
        low = n - 2 - k + (n - 1 - k - ep + n - 1) // n
        high = k + (k - ep + n) // n
        far_first.append((1 - upper) * low + upper * high)

    def ep_scatter(sem, send, recv, arrival=None):
        for j in far_first:
            remote(sem, send.at[j], recv.at[ep], (j, tp), arrival)

    others = pl.ds(0, n - 1)
    fellows = pl.ds(0, m - 1)
    groups = query_send.shape[0]
    s_first, s_plane, s_rows, s_proj = range(4)
    r_col, r_proj, r_side, r_back, r_near, r_query = range(6)
    r_reduce = r_query + groups
    r_mix = r_reduce + parts

    tokens_load.wait()
    rows_load.wait()
    attn_gain, mix_gain, branch_gate = (rows_ref[i] for i in range(3))
    stream = tokens_ref[...].astype(F32)
    normed = rms_scale(stream, attn_gain)
    for j in range(n):
        col_send[j] = normed[:, j * cols : (j + 1) * cols].astype(BF16)
    col_recv[ep] = col_send[ep]
    phase_name("barrier")
    pl.semaphore_wait(barrier, (n - 1) + (m - 1))
    phase_name("col_send")
    ep_scatter(s_first, col_send, col_recv, r_col)

    for copy in small_loads:
        copy.wait()
    later = lax.broadcasted_iota(jnp.int32, (slots, slots), 0) > lax.broadcasted_iota(
        jnp.int32, (slots, slots), 1
    )
    later = jnp.where(later, 1.0, 0.0).astype(BF16)
    capacity = mix_send.shape[2]
    lane_expert = lax.broadcasted_iota(jnp.int32, (seqs, n), 1).astype(F32)
    lane_slot = lax.broadcasted_iota(jnp.int32, (seqs, n * capacity), 1).astype(F32)
    row_slot = lax.broadcasted_iota(jnp.int32, (n * capacity, seqs), 0).astype(F32)
    first = lax.broadcasted_iota(jnp.int32, (seqs, seqs), 0)
    second = lax.broadcasted_iota(jnp.int32, (seqs, seqs), 1)
    weights = as_columns(weights_ref[...])
    ids = as_columns(ids_ref[...])
    named = [jnp.where(lane_expert == i, 1.0, 0.0) for i in ids]
    before = jnp.dot(
        jnp.where(second < first, 1.0, 0.0).astype(BF16),
        sum(named).astype(BF16),
        preferred_element_type=F32,
    )
    targets = [
        i * float(capacity) + jnp.sum(before * x, axis=1, keepdims=True) for i, x in zip(ids, named)
    ]
    route_map = jnp.concatenate(
        [jnp.where(lane_slot == t, 1.0, 0.0) for t in targets], axis=0
    ).astype(BF16)
    dispatch = sum(
        jnp.where(
            row_slot == jnp.sum(jnp.where(first == second, t, 0.0), axis=0, keepdims=True), 1.0, 0.0
        )
        for t in targets
    ).astype(BF16)
    proj_load.wait()
    phase_name("col_wait")
    arrived(r_col, col_recv.at[others])
    phase_name("project")
    picked = stack_rows(col_recv).astype(BF16)

    half = query_send.shape[3]
    part = jnp.dot(picked, proj_w[0], preferred_element_type=F32).astype(BF16)
    sent(s_first, col_send.at[others])
    for g in range(groups):
        for j in range(n):
            query_send[g, j] = part[j * seqs : (j + 1) * seqs, g * half : (g + 1) * half]
        query_recv[g, ep] = query_send[g, ep]
        ep_scatter(s_first, query_send.at[g], query_recv.at[g], r_query + g)
    phase_name("turn")
    out_load = load(0, out_w, (out_hbm, out_w))
    side_load = load(1, side_w, (side_gate_hbm, side_w.at[0]), (side_up_hbm, side_w.at[1]))
    side_down_load = load(2, side_down_w, (side_down_hbm, side_down_w))
    expert_load = load(3, expert_w, (gate_hbm.at[0], expert_w.at[0]), (up_hbm.at[0], expert_w.at[1]))
    down_load = load(4, down_w, (down_hbm.at[0], down_w))
    for i in (1, 2):
        part = jnp.dot(picked, proj_w[i], preferred_element_type=F32)
        for j in range(n):
            proj_send[i - 1, j] = part[j * seqs : (j + 1) * seqs].astype(BF16)
        proj_recv[i - 1, ep] = proj_send[i - 1, ep]
    key_load.wait()
    for s in range(seqs):
        for h in range(heads):
            turned[h, s] = keys[s, h].T
    value_load.wait()

    def collect(recv):
        total = recv[0].astype(F32)
        for j in range(1, n):
            total = total + recv[j].astype(F32)
        return total.astype(BF16).astype(F32)

    query_row = lax.broadcasted_iota(jnp.int32, (seqs, dh), 0)
    slot_row = lax.broadcasted_iota(jnp.int32, (seqs, slots), 0)
    position = lax.broadcasted_iota(jnp.int32, (seqs, slots), 1)
    lengths = as_columns(lengths_ref[...])[0].astype(jnp.int32)
    visible = position < lengths
    scale = dh ** (-0.5)
    some = half // dh
    score_rows, rest_rows = [], []
    for g in range(groups):
        phase_name("query_wait")
        arrived(r_query + g, query_recv.at[g, others])
        phase_name("scores")
        query = collect(query_recv.at[g])
        if g == 0:
            for i in range(2):
                ep_scatter(s_proj, proj_send.at[i], proj_recv.at[i], r_proj)
        for k in range(some):
            h = g * some + k
            q = rms_scale(query[:, k * dh : (k + 1) * dh], query_gain_ref[...])
            if k == some - 1:
                score = vector_products(q, turned.at[h])
            else:
                spread = jnp.concatenate(
                    [jnp.where(query_row == s, q, 0.0).astype(BF16) for s in range(seqs)], axis=1
                )
                score = jnp.dot(
                    spread, turned[h].reshape(seqs * dh, slots), preferred_element_type=F32
                )
            score = score * scale + bias_ref[0:1, h : h + 1]
            full = -softplus(score)
            score_rows.append(score + full)
            rest_rows.append(jnp.where(visible, full, 0.0))
    rest = jnp.concatenate(rest_rows, axis=0)
    high = rest.astype(BF16)
    left = rest - high.astype(F32)
    middle_part = left.astype(BF16)
    low = (left - middle_part.astype(F32)).astype(BF16)
    pieces = jnp.dot(
        jnp.concatenate([high, middle_part, low], axis=0), later, preferred_element_type=F32
    )
    count = seqs * heads
    between = pieces[:count] + pieces[count : 2 * count] + pieces[2 * count :]
    attended = []
    for h in range(heads):
        stick = jnp.where(
            visible, jnp.exp(score_rows[h] + between[h * seqs : (h + 1) * seqs]), 0.0
        )
        if h == 0:
            attended.append(vector_products(stick, values.at[h]))
            continue
        spread = jnp.concatenate(
            [jnp.where(slot_row == s, stick, 0.0).astype(BF16) for s in range(seqs)], axis=1
        )
        attended.append(
            jnp.dot(spread, values[h].reshape(seqs * slots, dh), preferred_element_type=F32)
        )
    attended = jnp.concatenate(attended, axis=1).astype(BF16)
    phase_name("out_proj")
    out_load.wait()
    for t in range(parts):
        reduce_buf[t, tp] = jnp.dot(
            attended, out_w[:, t * part_cols : (t + 1) * part_cols], preferred_element_type=F32
        ).astype(BF16)
        for d in range(1, m):
            own = reduce_buf.at[t, tp]
            remote(s_plane, own, own, (ep, lax.rem(tp + d, m)), r_reduce + t)

    middle = []
    for t in range(parts):
        phase_name("reduce_wait")
        arrived(r_reduce + t, reduce_buf.at[t, fellows])
        phase_name("mix")
        total = sum(reduce_buf[t, i].astype(F32) for i in range(m))
        part = (stream[:, t * part_cols : (t + 1) * part_cols] + total).astype(BF16)
        outbox = jnp.dot(dispatch, part, preferred_element_type=F32)
        for j in range(n):
            mix_send[t, j] = outbox[j * capacity : (j + 1) * capacity].astype(BF16)
        mix_recv[t, ep] = mix_send[t, ep]
        ep_scatter(s_rows, mix_send.at[t], mix_recv.at[t], r_mix + t)
        middle.append(part.astype(F32))
    middle = jnp.concatenate(middle, axis=1)
    for t in range(m):
        mid_cols[t] = middle[:, t * out_cols : (t + 1) * out_cols]

    phase_name("side")
    normed_mix = rms_scale(middle, mix_gain).astype(BF16)
    side_load.wait()
    side_down_load.wait()
    side_hidden = silu(
        jnp.dot(normed_mix, side_w[0], preferred_element_type=F32)
    ) * jnp.dot(normed_mix, side_w[1], preferred_element_type=F32)
    side_term = jnp.dot(side_hidden.astype(BF16), side_down_w[...], preferred_element_type=F32)
    switch = jnp.sum(normed_mix.astype(F32) * branch_gate, axis=1, keepdims=True)
    switch = 1.0 / (1.0 + jnp.exp(-switch))
    for t in range(m):
        side_cols[t] = switch * side_term[:, t * out_cols : (t + 1) * out_cols]
    sent(s_plane, reduce_buf.at[:, fellows])
    for d in range(1, m):
        t = lax.rem(tp + d, m)
        side_send[d - 1] = side_cols[t].astype(BF16)
        remote(s_plane, side_send.at[d - 1], side_recv.at[d - 1], (ep, t), r_side)

    phase_name("settle")
    expert_load.wait()
    down_load.wait()
    sent(s_first, query_send.at[:, others])

    squares = None
    for t in range(parts):
        phase_name("rows_wait")
        arrived(r_mix + t, mix_recv.at[t, others])
        phase_name("expert")
        for j in range(n):
            slot_rows[t, j * capacity : (j + 1) * capacity, :] = mix_recv[t, j].astype(F32)
        span = slice(t * part_cols, (t + 1) * part_cols)
        rows = slot_rows[t]
        square = jnp.sum(rows * rows, axis=1, keepdims=True)
        rows = (rows * mix_gain[:, span]).astype(BF16)
        for i in range(2):
            share = jnp.dot(rows, expert_w[i, span, :], preferred_element_type=F32)
            pre[i] = share if t == 0 else pre[i] + share
        squares = square if t == 0 else squares + square
        if t == 0:
            sent(s_plane, side_send.at[...])
    sent(s_rows, mix_send.at[:, others])
    gate_pre, up_pre = pre[0], pre[1]
    factor = lax.rsqrt(squares / width + epsilon)
    hidden = (silu(gate_pre * factor) * (up_pre * factor)).astype(BF16)
    for t in range(m):
        expert_term = jnp.dot(
            hidden, down_w[:, t * out_cols : (t + 1) * out_cols], preferred_element_type=F32
        )
        for j in range(n):
            back_send[t, j] = expert_term[j * capacity : (j + 1) * capacity].astype(BF16)
        for k in range(n - 1):
            j = k + (k - ep + n) // n
            remote(s_rows, back_send.at[t, j], back_recv.at[tp, ep], (j, t), r_back)
    for d in range(1, m):
        t = lax.rem(tp + d, m)
        remote(s_plane, back_send.at[t, ep], back_recv.at[tp, ep], (ep, t), r_near)
    back_recv[tp, ep] = back_send[tp, ep]
    phase_name("side_wait")
    result = mid_cols[tp] + side_cols[tp]
    arrived(r_side, side_recv.at[...])
    for d in range(1, m):
        result = result + side_recv[d - 1].astype(F32)
    phase_name("new_keys")
    arrived(r_proj, proj_recv.at[:, others])
    key_rows = collect(proj_recv.at[0])
    for h in range(heads):
        part = slice(h * dh, (h + 1) * dh)
        new_keys_ref[:, part] = rms_scale(key_rows[:, part], 1.0).astype(BF16)
    new_values_ref[...] = collect(proj_recv.at[1]).astype(BF16)
    sent(s_proj, proj_send.at[:, others])
    phase_name("back_wait")
    arrived(r_near, back_recv.at[fellows, 0])
    arrived(r_back, back_recv.at[:, others])
    phase_name("combine")
    for j in range(n):
        slot_cols[j * capacity : (j + 1) * capacity, :] = sum(
            back_recv[i, j].astype(F32) for i in range(m)
        )
    chosen = jnp.dot(route_map, slot_cols[...].astype(BF16), preferred_element_type=F32)
    for k, w in enumerate(weights):
        result = result + w * chosen[k * seqs : (k + 1) * seqs]
    mixed_ref[...] = result.astype(BF16)
    phase_name("drain")
    sent(s_plane, back_send.at[fellows, 0])
    sent(s_rows, back_send.at[:, others])
    phase_name(None)


def hand_on(count, *refs):
    sources, targets, sem = refs[:count], refs[count : 2 * count], refs[-1]
    copies = [
        pltpu.make_async_copy(src, dst, sem.at[i])
        for i, (src, dst) in enumerate(zip(sources, targets))
    ]
    for copy in copies:
        copy.start()
    for copy in copies:
        copy.wait()


def fused(n, m, *args):
    (
        tokens,
        attn_gain,
        query_weight,
        key_weight,
        value_weight,
        query_gain,
        stick_bias,
        key_cache,
        value_cache,
        lengths,
        out_weight,
        mix_gain,
        route_ids,
        route_weights,
        expert_gate,
        expert_up,
        expert_down,
        side_gate,
        side_up,
        side_down,
        branch_gate,
    ) = args
    seqs, width = tokens.shape
    _, heads, slots, dh = key_cache.shape
    head_cols = query_weight.shape[1]
    out_cols = width // m
    capacity = max(2, 2 * route_ids.shape[1] * seqs // n)
    parts = 2
    groups = 2
    vmem = pl.BlockSpec(memory_space=pltpu.VMEM)
    hbm = pl.BlockSpec(memory_space=pl.ANY)
    dma = pltpu.SemaphoreType.DMA

    def scratch(*shape, dtype=BF16):
        return pltpu.VMEM(shape, dtype)

    small = (
        tokens,
        attn_gain.reshape(1, width),
        query_gain.reshape(1, dh),
        stick_bias.reshape(1, heads),
        lengths.reshape(1, seqs),
        mix_gain.reshape(1, width),
        route_ids.T,
        route_weights.T,
        branch_gate.reshape(1, width),
    )
    shapes = ((seqs, out_cols), (seqs, head_cols), (seqs, head_cols))
    outs = pl.pallas_call(
        lambda *refs: layer_kernel(n, m, *refs),
        out_shape=tuple(pltpu.VMEM(shape, BF16) for shape in shapes),
        in_specs=[hbm] * 21,
        out_specs=(vmem, vmem, vmem),
        scratch_shapes=[
            scratch(seqs, width),
            scratch(3, 1, width, dtype=F32),
            *(scratch(*x.shape, dtype=x.dtype) for x in (*small[2:5], *small[6:8])),
            scratch(3, *query_weight.shape),
            scratch(*key_cache.shape),
            scratch(heads, seqs, dh, slots),
            scratch(heads, seqs, slots, dh),
            scratch(*out_weight.shape),
            scratch(2, *expert_gate.shape[1:]),
            scratch(*expert_down.shape[1:]),
            scratch(2, *side_gate.shape),
            scratch(*side_down.shape),
            scratch(n, seqs, width // n),
            scratch(n, seqs, width // n),
            scratch(groups, n, seqs, head_cols // groups),
            scratch(groups, n, seqs, head_cols // groups),
            scratch(2, n, seqs, head_cols),
            scratch(2, n, seqs, head_cols),
            scratch(parts, m, seqs, width // parts),
            scratch(m, seqs, out_cols, dtype=F32),
            scratch(parts, n, capacity, width // parts),
            scratch(parts, n, capacity, width // parts),
            scratch(parts, n * capacity, width // parts, dtype=F32),
            scratch(2, n * capacity, expert_gate.shape[2], dtype=F32),
            scratch(n * capacity, out_cols, dtype=F32),
            scratch(m, seqs, out_cols, dtype=F32),
            scratch(m - 1, seqs, out_cols),
            scratch(m - 1, seqs, out_cols),
            scratch(m, n, capacity, out_cols),
            scratch(m, n, capacity, out_cols),
            dma((10,)),
            dma((4,)),
            dma((5 + groups + 2 * parts,)),
        ],
        compiler_params=pltpu.CompilerParams(
            collective_id=0, has_side_effects=True, vmem_limit_bytes=60 * 1024 * 1024
        ),
        name="layer",
    )(
        *small,
        query_weight,
        key_weight,
        value_weight,
        key_cache,
        value_cache,
        out_weight,
        expert_gate,
        expert_up,
        expert_down,
        side_gate,
        side_up,
        side_down,
    )
    return pl.pallas_call(
        lambda *refs: hand_on(len(shapes), *refs),
        out_shape=tuple(jax.ShapeDtypeStruct(shape, BF16) for shape in shapes),
        in_specs=[vmem] * len(shapes),
        out_specs=(hbm,) * len(shapes),
        scratch_shapes=[dma((len(shapes),))],
        name="hand_on",
    )(*(pltpu.with_memory_space_constraint(x, pltpu.VMEM) for x in outs))


def layer(n, m, *args):
    tokens, query_weight, key_cache = args[0], args[2], args[7]
    expert_gate, side_gate = args[14], args[17]
    seqs, width = tokens.shape
    lanes = (width // n, width // m, query_weight.shape[1], key_cache.shape[2])
    lanes += (key_cache.shape[3], expert_gate.shape[2], side_gate.shape[1])
    lanes += (query_weight.shape[1] // 2, width // 2)
    rows = (seqs, key_cache.shape[1])
    held = 2 * sum(a.size for a in args[2:] if a.dtype == BF16) + 2 * key_cache.size
    aligned = all(x % 128 == 0 for x in lanes) and all(x % 8 == 0 for x in rows)
    if n > 1 and m > 1 and aligned and expert_gate.shape[0] == 1 and held < 48 * 1024 * 1024:
        return fused(n, m, *args)
    return body(*args)


def solution(mesh):
    in_specs = (
        P("ep", None),
        P(),
        P("ep", "tp"),
        P("ep", "tp"),
        P("ep", "tp"),
        P(),
        P("tp"),
        P("ep", "tp", None, None),
        P("ep", "tp", None, None),
        P("ep"),
        P("tp", None),
        P(),
        P("ep", None),
        P("ep", None),
        P("ep", None, "tp"),
        P("ep", None, "tp"),
        P("ep", "tp", None),
        P(None, "tp"),
        P(None, "tp"),
        P("tp", None),
        P(),
    )
    out_specs = (P("ep", "tp"), P("ep", "tp"), P("ep", "tp"))
    return jax.shard_map(
        lambda *args: layer(mesh.shape["ep"], mesh.shape["tp"], *args),
        mesh=mesh,
        in_specs=in_specs,
        out_specs=out_specs,
        check_vma=False,
    )
```

```python
import jax
import jax.numpy as jnp
from jax import lax
from jax.experimental import pallas as pl
from jax.experimental.pallas import tpu as pltpu
from jax.sharding import PartitionSpec as P

DH = 128


epsilon = 1e-06


def rms_scale(values, scale_gain):
    mean_square = jnp.mean(values * values, axis=-1, keepdims=True)
    return values * lax.rsqrt(mean_square + epsilon) * scale_gain


def body(
    tokens,
    attn_gain,
    query_weight,
    key_weight,
    value_weight,
    query_gain,
    stick_bias,
    key_cache,
    value_cache,
    lengths,
    out_weight,
    mix_gain,
    route_ids,
    route_weights,
    expert_gate,
    expert_up,
    expert_down,
    side_gate,
    side_up,
    side_down,
    branch_gate,
):
    seq_count, model_width = tokens.shape
    head_cols = query_weight.shape[1]
    heads_local = key_cache.shape[1]
    cache_slots = key_cache.shape[2]
    stream = tokens.astype(jnp.float32)
    normed = rms_scale(stream, attn_gain).astype(jnp.bfloat16)
    stacked = jnp.concatenate([query_weight, key_weight, value_weight], axis=1)
    columns = lax.all_to_all(normed, "ep", split_axis=1, concat_axis=0, tiled=True)
    picked = columns
    projected = lax.psum_scatter(
        jnp.dot(picked, stacked, preferred_element_type=jnp.float32),
        "ep",
        scatter_dimension=0,
        tiled=True,
    )
    query_rows = projected[:, :head_cols].astype(jnp.bfloat16)
    fresh_keys = projected[:, head_cols : 2 * head_cols].astype(jnp.bfloat16)
    new_values = projected[:, 2 * head_cols :].astype(jnp.bfloat16)
    new_keys = rms_scale(fresh_keys.astype(jnp.float32).reshape(seq_count, heads_local, DH), 1.0)
    new_keys = new_keys.astype(jnp.bfloat16).reshape(seq_count, head_cols)
    query_heads = rms_scale(
        query_rows.astype(jnp.float32).reshape(seq_count, heads_local, DH), query_gain
    )
    query_heads = query_heads.astype(jnp.bfloat16)
    scores = jnp.einsum("shd,shld->shl", query_heads, key_cache, preferred_element_type=jnp.float32)
    scores = scores * DH ** (-0.5) + stick_bias[None, :, None]
    positions = jnp.arange(cache_slots, dtype=jnp.int32)
    visible = positions[None, None, :] < lengths[:, None, None]
    log_rest = jnp.where(visible, jax.nn.log_sigmoid(-scores), 0.0)
    log_between = lax.cumsum(log_rest, axis=2, reverse=True) - log_rest
    stick = jnp.where(visible, jnp.exp(jax.nn.log_sigmoid(scores) + log_between), 0.0).astype(
        jnp.bfloat16
    )
    attended = jnp.einsum("shl,shld->shd", stick, value_cache, preferred_element_type=jnp.float32)
    attended = attended.astype(jnp.bfloat16).reshape(seq_count, head_cols)
    attn_proj = lax.psum(
        jnp.dot(attended, out_weight, preferred_element_type=jnp.float32).astype(jnp.bfloat16), "tp"
    ).astype(jnp.float32)
    middle = (stream + attn_proj).astype(jnp.bfloat16)
    normed_mix = rms_scale(middle.astype(jnp.float32), mix_gain).astype(jnp.bfloat16)
    side_gate_pre = jnp.dot(normed_mix, side_gate, preferred_element_type=jnp.float32)
    side_up_pre = jnp.dot(normed_mix, side_up, preferred_element_type=jnp.float32)
    side_hidden = (jax.nn.silu(side_gate_pre) * side_up_pre).astype(jnp.bfloat16)
    side_term = jnp.dot(side_hidden, side_down, preferred_element_type=jnp.float32)
    switch = jax.nn.sigmoid(
        jnp.sum(normed_mix.astype(jnp.float32) * branch_gate, axis=1, keepdims=True)
    )
    experts = lax.axis_size("ep")
    top_count = route_ids.shape[1]
    capacity = max(2, 2 * top_count * seq_count // experts)
    flat_ids = route_ids.reshape(-1)
    onehot = (flat_ids[:, None] == jnp.arange(experts, dtype=jnp.int32)[None, :]).astype(jnp.int32)
    before = jnp.cumsum(onehot, axis=0) - onehot
    slot_index = jnp.sum(before * onehot, axis=1)
    target = flat_ids * capacity + slot_index
    route_map = (
        target[:, None] == jnp.arange(experts * capacity, dtype=jnp.int32)[None, :]
    ).astype(jnp.bfloat16)
    dispatch = jnp.sum(route_map.reshape(seq_count, top_count, experts * capacity), axis=1).T
    outbox = jnp.dot(dispatch, normed_mix, preferred_element_type=jnp.float32).astype(jnp.bfloat16)
    outbox = outbox.reshape(experts, capacity, model_width)
    col_width = model_width // lax.axis_size("tp")
    col_offset = lax.axis_index("tp") * col_width
    arrived = lax.all_to_all(outbox, "ep", split_axis=0, concat_axis=0, tiled=True)
    slot_rows = arrived.reshape(experts * capacity, model_width)
    gate_pre = jnp.dot(slot_rows, expert_gate[0], preferred_element_type=jnp.float32)
    up_pre = jnp.dot(slot_rows, expert_up[0], preferred_element_type=jnp.float32)
    hidden = (jax.nn.silu(gate_pre) * up_pre).astype(jnp.bfloat16)
    expert_term = jnp.dot(hidden, expert_down[0], preferred_element_type=jnp.float32)
    expert_part, side_part = (
        lax.psum_scatter(
            expert_term.astype(jnp.bfloat16), "tp", scatter_dimension=1, tiled=True
        ).astype(jnp.float32),
        lax.psum_scatter(
            side_term.astype(jnp.bfloat16), "tp", scatter_dimension=1, tiled=True
        ).astype(jnp.float32),
    )
    returned = lax.all_to_all(
        expert_part.astype(jnp.bfloat16).reshape(experts, capacity, col_width),
        "ep",
        split_axis=0,
        concat_axis=0,
        tiled=True,
    )
    picked = jnp.dot(
        route_map,
        returned.reshape(experts * capacity, col_width),
        preferred_element_type=jnp.float32,
    )
    routed = jnp.sum(
        route_weights[:, :, None] * picked.reshape(seq_count, top_count, col_width), axis=1
    )
    middle_cols = lax.dynamic_slice_in_dim(middle, col_offset, col_width, 1).astype(jnp.float32)
    mixed = (middle_cols + routed + switch * side_part).astype(jnp.bfloat16)
    return (mixed, new_keys, new_values)


MESH = pl.DeviceIdType.MESH
F32 = jnp.float32
BF16 = jnp.bfloat16


def softplus(values):
    return jnp.maximum(values, 0.0) + jnp.log1p(jnp.exp(-jnp.abs(values)))


def silu(values):
    return values / (1.0 + jnp.exp(-values))


def as_columns(rows):
    count = rows.shape[1]
    own = lax.broadcasted_iota(jnp.int32, (count, count), 0) == lax.broadcasted_iota(
        jnp.int32, (count, count), 1
    )
    rows = rows.astype(F32)
    return [
        jnp.sum(jnp.where(own, rows[i : i + 1], 0.0), axis=1, keepdims=True)
        for i in range(rows.shape[0])
    ]


class Phases:
    def __init__(self):
        self.scope = None

    def __call__(self, name):
        if self.scope is not None:
            self.scope.__exit__(None, None, None)
        self.scope = jax.named_scope(name) if name else None
        if self.scope is not None:
            self.scope.__enter__()


def stack_rows(buffer):
    return jnp.concatenate([buffer[i].astype(F32) for i in range(buffer.shape[0])], axis=0)


def vector_products(rows, blocks):
    columns = rows.astype(BF16).astype(F32).T
    return jnp.concatenate(
        [
            jnp.sum(blocks[s].astype(F32) * columns[:, s : s + 1], axis=0, keepdims=True)
            for s in range(rows.shape[0])
        ],
        axis=0,
    )


def layer_kernel(
    n,
    m,
    tokens_hbm,
    attn_gain_hbm,
    query_gain_hbm,
    bias_hbm,
    lengths_hbm,
    mix_gain_hbm,
    ids_hbm,
    weights_hbm,
    branch_hbm,
    wq_hbm,
    wk_hbm,
    wv_hbm,
    key_hbm,
    value_hbm,
    out_hbm,
    gate_hbm,
    up_hbm,
    down_hbm,
    side_gate_hbm,
    side_up_hbm,
    side_down_hbm,
    mixed_ref,
    new_keys_ref,
    new_values_ref,
    tokens_ref,
    rows_ref,
    query_gain_ref,
    bias_ref,
    lengths_ref,
    ids_ref,
    weights_ref,
    proj_w,
    keys,
    turned,
    values,
    out_w,
    expert_w,
    down_w,
    side_w,
    side_down_w,
    col_send,
    col_recv,
    query_send,
    query_recv,
    proj_send,
    proj_recv,
    reduce_buf,
    mid_cols,
    mix_send,
    mix_recv,
    slot_rows,
    pre,
    slot_cols,
    side_cols,
    side_send,
    side_recv,
    back_send,
    back_recv,
    load_sem,
    send_sem,
    recv_sem,
):
    ep = lax.axis_index("ep")
    tp = lax.axis_index("tp")
    seqs, width = tokens_ref.shape
    heads, dh, slots = turned.shape[0], turned.shape[2], turned.shape[3]
    cols = width // n
    out_cols = width // m
    parts = reduce_buf.shape[0]
    part_cols = width // parts

    phase_name = Phases()
    phase_name("greet")
    def load(k, whole, *pairs, priority=1):
        for src, dst in pairs:
            pltpu.make_async_copy(src, dst, load_sem.at[k]).start(priority=priority)
        return pltpu.make_async_copy(whole, whole, load_sem.at[k])

    tokens_load = load(0, tokens_ref, (tokens_hbm, tokens_ref), priority=0)
    gains = (attn_gain_hbm, mix_gain_hbm, branch_hbm)
    rows_load = load(1, rows_ref, *((x, rows_ref.at[i]) for i, x in enumerate(gains)), priority=0)
    barrier = pltpu.get_barrier_semaphore()
    for d in range(1, n):
        pl.semaphore_signal(barrier, inc=1, device_id=(lax.rem(ep + d, n), tp), device_id_type=MESH)
    for d in range(1, m):
        pl.semaphore_signal(barrier, inc=1, device_id=(ep, lax.rem(tp + d, m)), device_id_type=MESH)
    small = (
        (ids_hbm, ids_ref),
        (weights_hbm, weights_ref),
        (query_gain_hbm, query_gain_ref),
        (bias_hbm, bias_ref),
        (lengths_hbm, lengths_ref),
    )
    small_loads = [load(2 + i, x[1], x, priority=0) for i, x in enumerate(small)]
    proj_load = load(
        7,
        proj_w,
        *((w, proj_w.at[i]) for i, w in enumerate((wq_hbm, wk_hbm, wv_hbm))),
        priority=0,
    )
    key_load = load(8, keys, *((key_hbm.at[i], keys.at[i]) for i in range(seqs)))
    value_load = load(9, values, *((value_hbm.at[i], values.at[:, i]) for i in range(seqs)))

    def remote(sem, src, dst, target, arrival=None):
        copy = pltpu.make_async_remote_copy(
            src_ref=src,
            dst_ref=dst,
            send_sem=send_sem.at[sem],
            recv_sem=recv_sem.at[sem if arrival is None else arrival],
            device_id=target,
            device_id_type=MESH,
        )
        copy.start()

    def sent(sem, whole):
        pltpu.make_async_copy(whole, whole, send_sem.at[sem]).wait()

    def arrived(sem, whole):
        pltpu.make_async_copy(whole, whole, recv_sem.at[sem]).wait()

    upper = ep // (n // 2)
    far_first = []
    for k in range(n - 1):
        low = n - 2 - k + (n - 1 - k - ep + n - 1) // n
        high = k + (k - ep + n) // n
        far_first.append((1 - upper) * low + upper * high)

    def ep_scatter(sem, send, recv, arrival=None):
        for j in far_first:
            remote(sem, send.at[j], recv.at[ep], (j, tp), arrival)

    others = pl.ds(0, n - 1)
    fellows = pl.ds(0, m - 1)
    groups = query_send.shape[0]
    s_first, s_plane, s_rows, s_proj = range(4)
    r_col, r_proj, r_side, r_back, r_near, r_query = range(6)
    r_reduce = r_query + groups
    r_mix = r_reduce + parts

    tokens_load.wait()
    rows_load.wait()
    attn_gain, mix_gain, branch_gate = (rows_ref[i] for i in range(3))
    stream = tokens_ref[...].astype(F32)
    normed = rms_scale(stream, attn_gain)
    for j in range(n):
        col_send[j] = normed[:, j * cols : (j + 1) * cols].astype(BF16)
    col_recv[ep] = col_send[ep]
    phase_name("barrier")
    pl.semaphore_wait(barrier, (n - 1) + (m - 1))
    phase_name("col_send")
    ep_scatter(s_first, col_send, col_recv, r_col)

    for copy in small_loads:
        copy.wait()
    later = lax.broadcasted_iota(jnp.int32, (slots, slots), 0) > lax.broadcasted_iota(
        jnp.int32, (slots, slots), 1
    )
    later = jnp.where(later, 1.0, 0.0).astype(BF16)
    capacity = mix_send.shape[2]
    lane_expert = lax.broadcasted_iota(jnp.int32, (seqs, n), 1).astype(F32)
    lane_slot = lax.broadcasted_iota(jnp.int32, (seqs, n * capacity), 1).astype(F32)
    row_slot = lax.broadcasted_iota(jnp.int32, (n * capacity, seqs), 0).astype(F32)
    first = lax.broadcasted_iota(jnp.int32, (seqs, seqs), 0)
    second = lax.broadcasted_iota(jnp.int32, (seqs, seqs), 1)
    weights = as_columns(weights_ref[...])
    ids = as_columns(ids_ref[...])
    named = [jnp.where(lane_expert == i, 1.0, 0.0) for i in ids]
    before = jnp.dot(
        jnp.where(second < first, 1.0, 0.0).astype(BF16),
        sum(named).astype(BF16),
        preferred_element_type=F32,
    )
    targets = [
        i * float(capacity) + jnp.sum(before * x, axis=1, keepdims=True) for i, x in zip(ids, named)
    ]
    route_map = jnp.concatenate(
        [jnp.where(lane_slot == t, 1.0, 0.0) for t in targets], axis=0
    ).astype(BF16)
    dispatch = sum(
        jnp.where(
            row_slot == jnp.sum(jnp.where(first == second, t, 0.0), axis=0, keepdims=True), 1.0, 0.0
        )
        for t in targets
    ).astype(BF16)
    proj_load.wait()
    phase_name("col_wait")
    arrived(r_col, col_recv.at[others])
    phase_name("project")
    picked = stack_rows(col_recv).astype(BF16)

    half = query_send.shape[3]
    part = jnp.dot(picked, proj_w[0], preferred_element_type=F32).astype(BF16)
    sent(s_first, col_send.at[others])
    for g in range(groups):
        for j in range(n):
            query_send[g, j] = part[j * seqs : (j + 1) * seqs, g * half : (g + 1) * half]
        query_recv[g, ep] = query_send[g, ep]
        ep_scatter(s_first, query_send.at[g], query_recv.at[g], r_query + g)
    phase_name("turn")
    out_load = load(0, out_w, (out_hbm, out_w))
    side_load = load(1, side_w, (side_gate_hbm, side_w.at[0]), (side_up_hbm, side_w.at[1]))
    side_down_load = load(2, side_down_w, (side_down_hbm, side_down_w))
    expert_load = load(3, expert_w, (gate_hbm.at[0], expert_w.at[0]), (up_hbm.at[0], expert_w.at[1]))
    down_load = load(4, down_w, (down_hbm.at[0], down_w))
    for i in (1, 2):
        part = jnp.dot(picked, proj_w[i], preferred_element_type=F32)
        for j in range(n):
            proj_send[i - 1, j] = part[j * seqs : (j + 1) * seqs].astype(BF16)
        proj_recv[i - 1, ep] = proj_send[i - 1, ep]
    key_load.wait()
    for s in range(seqs):
        for h in range(heads):
            turned[h, s] = keys[s, h].T
    value_load.wait()

    def collect(recv):
        total = recv[0].astype(F32)
        for j in range(1, n):
            total = total + recv[j].astype(F32)
        return total.astype(BF16).astype(F32)

    query_row = lax.broadcasted_iota(jnp.int32, (seqs, dh), 0)
    slot_row = lax.broadcasted_iota(jnp.int32, (seqs, slots), 0)
    position = lax.broadcasted_iota(jnp.int32, (seqs, slots), 1)
    lengths = as_columns(lengths_ref[...])[0].astype(jnp.int32)
    visible = position < lengths
    scale = dh ** (-0.5)
    some = half // dh
    score_rows, rest_rows = [], []
    for g in range(groups):
        phase_name("query_wait")
        arrived(r_query + g, query_recv.at[g, others])
        phase_name("scores")
        query = collect(query_recv.at[g])
        if g == 0:
            for i in range(2):
                ep_scatter(s_proj, proj_send.at[i], proj_recv.at[i], r_proj)
        for k in range(some):
            h = g * some + k
            q = rms_scale(query[:, k * dh : (k + 1) * dh], query_gain_ref[...])
            if k == some - 1:
                score = vector_products(q, turned.at[h])
            else:
                spread = jnp.concatenate(
                    [jnp.where(query_row == s, q, 0.0).astype(BF16) for s in range(seqs)], axis=1
                )
                score = jnp.dot(
                    spread, turned[h].reshape(seqs * dh, slots), preferred_element_type=F32
                )
            score = score * scale + bias_ref[0:1, h : h + 1]
            full = -softplus(score)
            score_rows.append(score + full)
            rest_rows.append(jnp.where(visible, full, 0.0))
    rest = jnp.concatenate(rest_rows, axis=0)
    high = rest.astype(BF16)
    low = (rest - high.astype(F32)).astype(BF16)
    pieces = jnp.dot(
        jnp.concatenate([high, low], axis=0), later, preferred_element_type=F32
    )
    count = seqs * heads
    between = pieces[:count] + pieces[count:]
    attended = []
    for h in range(heads):
        stick = jnp.where(
            visible, jnp.exp(score_rows[h] + between[h * seqs : (h + 1) * seqs]), 0.0
        )
        if h == 0:
            attended.append(vector_products(stick, values.at[h]))
            continue
        spread = jnp.concatenate(
            [jnp.where(slot_row == s, stick, 0.0).astype(BF16) for s in range(seqs)], axis=1
        )
        attended.append(
            jnp.dot(spread, values[h].reshape(seqs * slots, dh), preferred_element_type=F32)
        )
    attended = jnp.concatenate(attended, axis=1).astype(BF16)
    phase_name("out_proj")
    out_load.wait()
    for t in range(parts):
        reduce_buf[t, tp] = jnp.dot(
            attended, out_w[:, t * part_cols : (t + 1) * part_cols], preferred_element_type=F32
        ).astype(BF16)
        for d in range(1, m):
            own = reduce_buf.at[t, tp]
            remote(s_plane, own, own, (ep, lax.rem(tp + d, m)), r_reduce + t)

    middle = []
    for t in range(parts):
        phase_name("reduce_wait")
        arrived(r_reduce + t, reduce_buf.at[t, fellows])
        phase_name("mix")
        total = sum(reduce_buf[t, i].astype(F32) for i in range(m))
        part = (stream[:, t * part_cols : (t + 1) * part_cols] + total).astype(BF16)
        outbox = jnp.dot(dispatch, part, preferred_element_type=F32)
        for j in range(n):
            mix_send[t, j] = outbox[j * capacity : (j + 1) * capacity].astype(BF16)
        mix_recv[t, ep] = mix_send[t, ep]
        ep_scatter(s_rows, mix_send.at[t], mix_recv.at[t], r_mix + t)
        middle.append(part.astype(F32))
    middle = jnp.concatenate(middle, axis=1)
    for t in range(m):
        mid_cols[t] = middle[:, t * out_cols : (t + 1) * out_cols]

    phase_name("side")
    normed_mix = rms_scale(middle, mix_gain).astype(BF16)
    side_load.wait()
    side_down_load.wait()
    side_hidden = silu(
        jnp.dot(normed_mix, side_w[0], preferred_element_type=F32)
    ) * jnp.dot(normed_mix, side_w[1], preferred_element_type=F32)
    side_term = jnp.dot(side_hidden.astype(BF16), side_down_w[...], preferred_element_type=F32)
    switch = jnp.sum(normed_mix.astype(F32) * branch_gate, axis=1, keepdims=True)
    switch = 1.0 / (1.0 + jnp.exp(-switch))
    for t in range(m):
        side_cols[t] = switch * side_term[:, t * out_cols : (t + 1) * out_cols]
    sent(s_plane, reduce_buf.at[:, fellows])
    for d in range(1, m):
        t = lax.rem(tp + d, m)
        side_send[d - 1] = side_cols[t].astype(BF16)
        remote(s_plane, side_send.at[d - 1], side_recv.at[d - 1], (ep, t), r_side)

    phase_name("settle")
    expert_load.wait()
    down_load.wait()
    sent(s_first, query_send.at[:, others])

    squares = None
    for t in range(parts):
        phase_name("rows_wait")
        arrived(r_mix + t, mix_recv.at[t, others])
        phase_name("expert")
        for j in range(n):
            slot_rows[t, j * capacity : (j + 1) * capacity, :] = mix_recv[t, j].astype(F32)
        span = slice(t * part_cols, (t + 1) * part_cols)
        rows = slot_rows[t]
        square = jnp.sum(rows * rows, axis=1, keepdims=True)
        rows = (rows * mix_gain[:, span]).astype(BF16)
        for i in range(2):
            share = jnp.dot(rows, expert_w[i, span, :], preferred_element_type=F32)
            pre[i] = share if t == 0 else pre[i] + share
        squares = square if t == 0 else squares + square
        if t == 0:
            sent(s_plane, side_send.at[...])
    sent(s_rows, mix_send.at[:, others])
    gate_pre, up_pre = pre[0], pre[1]
    factor = lax.rsqrt(squares / width + epsilon)
    hidden = (silu(gate_pre * factor) * (up_pre * factor)).astype(BF16)
    for t in range(m):
        expert_term = jnp.dot(
            hidden, down_w[:, t * out_cols : (t + 1) * out_cols], preferred_element_type=F32
        )
        for j in range(n):
            back_send[t, j] = expert_term[j * capacity : (j + 1) * capacity].astype(BF16)
        for k in range(n - 1):
            j = k + (k - ep + n) // n
            remote(s_rows, back_send.at[t, j], back_recv.at[tp, ep], (j, t), r_back)
    for d in range(1, m):
        t = lax.rem(tp + d, m)
        remote(s_plane, back_send.at[t, ep], back_recv.at[tp, ep], (ep, t), r_near)
    back_recv[tp, ep] = back_send[tp, ep]
    phase_name("side_wait")
    result = mid_cols[tp] + side_cols[tp]
    arrived(r_side, side_recv.at[...])
    for d in range(1, m):
        result = result + side_recv[d - 1].astype(F32)
    phase_name("new_keys")
    arrived(r_proj, proj_recv.at[:, others])
    key_rows = collect(proj_recv.at[0])
    for h in range(heads):
        part = slice(h * dh, (h + 1) * dh)
        new_keys_ref[:, part] = rms_scale(key_rows[:, part], 1.0).astype(BF16)
    new_values_ref[...] = collect(proj_recv.at[1]).astype(BF16)
    sent(s_proj, proj_send.at[:, others])
    phase_name("back_wait")
    arrived(r_near, back_recv.at[fellows, 0])
    arrived(r_back, back_recv.at[:, others])
    phase_name("combine")
    for j in range(n):
        slot_cols[j * capacity : (j + 1) * capacity, :] = sum(
            back_recv[i, j].astype(F32) for i in range(m)
        )
    chosen = jnp.dot(route_map, slot_cols[...].astype(BF16), preferred_element_type=F32)
    for k, w in enumerate(weights):
        result = result + w * chosen[k * seqs : (k + 1) * seqs]
    mixed_ref[...] = result.astype(BF16)
    phase_name("drain")
    sent(s_plane, back_send.at[fellows, 0])
    sent(s_rows, back_send.at[:, others])
    phase_name(None)


def hand_on(count, *refs):
    sources, targets, sem = refs[:count], refs[count : 2 * count], refs[-1]
    copies = [
        pltpu.make_async_copy(src, dst, sem.at[i])
        for i, (src, dst) in enumerate(zip(sources, targets))
    ]
    for copy in copies:
        copy.start()
    for copy in copies:
        copy.wait()


def fused(n, m, *args):
    (
        tokens,
        attn_gain,
        query_weight,
        key_weight,
        value_weight,
        query_gain,
        stick_bias,
        key_cache,
        value_cache,
        lengths,
        out_weight,
        mix_gain,
        route_ids,
        route_weights,
        expert_gate,
        expert_up,
        expert_down,
        side_gate,
        side_up,
        side_down,
        branch_gate,
    ) = args
    seqs, width = tokens.shape
    _, heads, slots, dh = key_cache.shape
    head_cols = query_weight.shape[1]
    out_cols = width // m
    capacity = max(2, 2 * route_ids.shape[1] * seqs // n)
    parts = 2
    groups = 2
    vmem = pl.BlockSpec(memory_space=pltpu.VMEM)
    hbm = pl.BlockSpec(memory_space=pl.ANY)
    dma = pltpu.SemaphoreType.DMA

    def scratch(*shape, dtype=BF16):
        return pltpu.VMEM(shape, dtype)

    small = (
        tokens,
        attn_gain.reshape(1, width),
        query_gain.reshape(1, dh),
        stick_bias.reshape(1, heads),
        lengths.reshape(1, seqs),
        mix_gain.reshape(1, width),
        route_ids.T,
        route_weights.T,
        branch_gate.reshape(1, width),
    )
    shapes = ((seqs, out_cols), (seqs, head_cols), (seqs, head_cols))
    outs = pl.pallas_call(
        lambda *refs: layer_kernel(n, m, *refs),
        out_shape=tuple(pltpu.VMEM(shape, BF16) for shape in shapes),
        in_specs=[hbm] * 21,
        out_specs=(vmem, vmem, vmem),
        scratch_shapes=[
            scratch(seqs, width),
            scratch(3, 1, width, dtype=F32),
            *(scratch(*x.shape, dtype=x.dtype) for x in (*small[2:5], *small[6:8])),
            scratch(3, *query_weight.shape),
            scratch(*key_cache.shape),
            scratch(heads, seqs, dh, slots),
            scratch(heads, seqs, slots, dh),
            scratch(*out_weight.shape),
            scratch(2, *expert_gate.shape[1:]),
            scratch(*expert_down.shape[1:]),
            scratch(2, *side_gate.shape),
            scratch(*side_down.shape),
            scratch(n, seqs, width // n),
            scratch(n, seqs, width // n),
            scratch(groups, n, seqs, head_cols // groups),
            scratch(groups, n, seqs, head_cols // groups),
            scratch(2, n, seqs, head_cols),
            scratch(2, n, seqs, head_cols),
            scratch(parts, m, seqs, width // parts),
            scratch(m, seqs, out_cols, dtype=F32),
            scratch(parts, n, capacity, width // parts),
            scratch(parts, n, capacity, width // parts),
            scratch(parts, n * capacity, width // parts, dtype=F32),
            scratch(2, n * capacity, expert_gate.shape[2], dtype=F32),
            scratch(n * capacity, out_cols, dtype=F32),
            scratch(m, seqs, out_cols, dtype=F32),
            scratch(m - 1, seqs, out_cols),
            scratch(m - 1, seqs, out_cols),
            scratch(m, n, capacity, out_cols),
            scratch(m, n, capacity, out_cols),
            dma((10,)),
            dma((4,)),
            dma((5 + groups + 2 * parts,)),
        ],
        compiler_params=pltpu.CompilerParams(
            collective_id=0, has_side_effects=True, vmem_limit_bytes=60 * 1024 * 1024
        ),
        name="layer",
    )(
        *small,
        query_weight,
        key_weight,
        value_weight,
        key_cache,
        value_cache,
        out_weight,
        expert_gate,
        expert_up,
        expert_down,
        side_gate,
        side_up,
        side_down,
    )
    return pl.pallas_call(
        lambda *refs: hand_on(len(shapes), *refs),
        out_shape=tuple(jax.ShapeDtypeStruct(shape, BF16) for shape in shapes),
        in_specs=[vmem] * len(shapes),
        out_specs=(hbm,) * len(shapes),
        scratch_shapes=[dma((len(shapes),))],
        name="hand_on",
    )(*(pltpu.with_memory_space_constraint(x, pltpu.VMEM) for x in outs))


def layer(n, m, *args):
    tokens, query_weight, key_cache = args[0], args[2], args[7]
    expert_gate, side_gate = args[14], args[17]
    seqs, width = tokens.shape
    lanes = (width // n, width // m, query_weight.shape[1], key_cache.shape[2])
    lanes += (key_cache.shape[3], expert_gate.shape[2], side_gate.shape[1])
    lanes += (query_weight.shape[1] // 2, width // 2)
    rows = (seqs, key_cache.shape[1])
    held = 2 * sum(a.size for a in args[2:] if a.dtype == BF16) + 2 * key_cache.size
    aligned = all(x % 128 == 0 for x in lanes) and all(x % 8 == 0 for x in rows)
    if n > 1 and m > 1 and aligned and expert_gate.shape[0] == 1 and held < 48 * 1024 * 1024:
        return fused(n, m, *args)
    return body(*args)


def solution(mesh):
    in_specs = (
        P("ep", None),
        P(),
        P("ep", "tp"),
        P("ep", "tp"),
        P("ep", "tp"),
        P(),
        P("tp"),
        P("ep", "tp", None, None),
        P("ep", "tp", None, None),
        P("ep"),
        P("tp", None),
        P(),
        P("ep", None),
        P("ep", None),
        P("ep", None, "tp"),
        P("ep", None, "tp"),
        P("ep", "tp", None),
        P(None, "tp"),
        P(None, "tp"),
        P("tp", None),
        P(),
    )
    out_specs = (P("ep", "tp"), P("ep", "tp"), P("ep", "tp"))
    return jax.shard_map(
        lambda *args: layer(mesh.shape["ep"], mesh.shape["tp"], *args),
        mesh=mesh,
        in_specs=in_specs,
        out_specs=out_specs,
        check_vma=False,
    )
```
